512 devices in a mesh: kv: 64 (over z, y), tp: 8 (over x, core).
Axes of the slice: x: 4, y: 8, z: 8, core: 2. Of those that a mesh axis runs over, the one named last changes fastest.
Arguments:
- tokens: bfloat16 [256, 4, 2048], P('kv', None, 'tp'), may hold values from -6 to 6
- input_gain: float32 [2048], replicated, may hold values from 0.1 to 1.9
- gate_weight: bfloat16 [2048, 4096], P('kv', 'tp'), may hold values from -0.125 to 0.125
- value_weight: bfloat16 [2048, 4096], P('kv', 'tp'), may hold values from -0.125 to 0.125
- write_weight: bfloat16 [2048, 1024], P('kv', 'tp'), may hold values from -0.125 to 0.125
- read_weight: bfloat16 [2048, 1024], P('kv', 'tp'), may hold values from -0.125 to 0.125
- step_weight: bfloat16 [2048, 64], replicated, may hold values from -0.125 to 0.125
- conv_value: float32 [4, 4096], P(None, 'tp'), may hold values from -3 to 3
- conv_write: float32 [4, 1024], P(None, 'tp'), may hold values from -3 to 3
- conv_read: float32 [4, 1024], P(None, 'tp'), may hold values from -3 to 3
- step_bias: float32 [64], P('tp'), may hold values from -4 to -1
- decay_log: float32 [64], P('tp'), may hold values from 0 to 2.8
- skip_gain: float32 [64], P('tp'), may hold values from 0.5 to 1.5
- output_gain: float32 [4096], P('tp'), may hold values from 0.1 to 1.9
- out_weight: bfloat16 [4096, 2048], P('tp', 'kv'), may hold values from -0.09375 to 0.09375
- base_state: float32 [256, 64, 64, 128], P('kv', 'tp'), may hold values from -2 to 2
- past_value: bfloat16 [256, 7, 4096], P('kv', None, 'tp'), may hold values from -6 to 6
- past_write: bfloat16 [256, 7, 1024], P('kv', None, 'tp'), may hold values from -6 to 6
- past_read: bfloat16 [256, 7, 1024], P('kv', None, 'tp'), may hold values from -6 to 6
- past_step: bfloat16 [256, 4, 64], P('kv', None, 'tp'), may hold values from -4 to 4
- accepted: int32 [256], P('kv'), may hold values from 1 to 4
Outputs:
- mixed: bfloat16 [256, 4, 2048], P('kv', None, 'tp')
- root_state: float32 [256, 64, 64, 128], P('kv', 'tp')
- next_value: bfloat16 [256, 7, 4096], P('kv', None, 'tp')
- next_write: bfloat16 [256, 7, 1024], P('kv', None, 'tp')
- next_read: bfloat16 [256, 7, 1024], P('kv', None, 'tp')
- next_step: bfloat16 [256, 4, 64], P('kv', None, 'tp')
The draws below stay inside these ranges and needn't reach their ends.
Inputs may be any that keep to these rules, and one draw needn't show every extreme that they name: Every entry of `accepted` is an integer from 1 to 4 (at least one of the last step's proposals is always accepted).
All inputs are finite; a program needn't handle non-finite values.
Results may differ from the reference program's by a relative error of at most 0.018.
Values may be sent and summed in bfloat16 or wider, within the bound.
A program may use at most 64 MiB of HBM per device.

```python
import jax
import jax.numpy as jnp
from jax import lax

WIDTH = 2048
INNER = 4096
HEADS = 64
HEAD_DIM = 64
GROUPS = 8
STATE_DIM = 128
CONV_W = 4
PROPOSALS = 4
SEQS = 256
PAST_ROWS = 7
N_TP = 8


def plant(entries, key, smallest, high):
    dims = entries.shape
    spot = [jax.random.randint(jax.random.fold_in(key, axis), (), 0, dims[axis]) for axis in range(len(dims))]
    entries = entries.at[tuple(spot)].set(smallest)
    longest = dims.index(max(dims))
    spot[longest] = (spot[longest] + 1) % dims[longest]
    return entries.at[tuple(spot)].set(high)


def levels(stream_key, shape, pieces, low, high):
    level = 1.0
    for dim, parts in pieces:
        draws = jax.random.uniform(jax.random.fold_in(jax.random.fold_in(stream_key, 6), dim), (parts,), jnp.float32, low / len(pieces), high / len(pieces))
        level = level * jnp.repeat(jnp.exp(draws), shape[dim] // parts).reshape((-1,) + (1,) * (len(shape) - 1 - dim))
    return level


def noise(key, extent, scale, most, shards=(), kind=jnp.bfloat16):
    loudness = levels(key, extent, shards, -0.22, 0.18) if shards else 1.0
    values = jax.random.normal(key, extent, jnp.float32) * scale * loudness
    return jnp.minimum(jnp.maximum(values, -most), most).astype(kind)


def setup_inputs(seed: int = 0) -> dict:
    key_of = jax.random.split(jax.random.key(seed), 22)
    tokens = noise(key_of[0], (SEQS, PROPOSALS, WIDTH), 1.0, 6.0, ((0, 64), (2, 8)))
    input_gain = jnp.clip(1.0 + 0.18 * jax.random.normal(key_of[1], (WIDTH,), jnp.float32), 0.1, 1.9)
    gate_weight = noise(key_of[2], (WIDTH, INNER), WIDTH ** -0.5, 0.125, ((0, 64), (1, 8)))
    value_weight = noise(key_of[3], (WIDTH, INNER), WIDTH ** -0.5, 0.125, ((0, 64), (1, 8)))
    write_weight = noise(key_of[4], (WIDTH, GROUPS * STATE_DIM), WIDTH ** -0.5, 0.125, ((0, 64), (1, 8)))
    read_weight = noise(key_of[5], (WIDTH, GROUPS * STATE_DIM), WIDTH ** -0.5, 0.125, ((0, 64), (1, 8)))
    step_weight = noise(key_of[6], (WIDTH, HEADS), WIDTH ** -0.5, 0.125)
    conv_value = noise(key_of[7], (CONV_W, INNER), 0.5, 3.0, ((1, 8),), jnp.float32)
    conv_write = noise(key_of[8], (CONV_W, GROUPS * STATE_DIM), 0.5, 3.0, ((1, 8),), jnp.float32)
    conv_read = noise(key_of[9], (CONV_W, GROUPS * STATE_DIM), 0.5, 3.0, ((1, 8),), jnp.float32)
    step_bias = jnp.clip(-4.0 + 3.0 * jax.random.uniform(key_of[10], (HEADS,), jnp.float32) ** levels(key_of[10], (HEADS,), ((0, 8),), -0.2, 0.2), -4.0, -1.0)
    decay_log = jnp.clip(2.8 * jax.random.uniform(key_of[11], (HEADS,), jnp.float32) ** levels(key_of[11], (HEADS,), ((0, 8),), -0.2, 0.2), 0.0, 2.8)
    skip_gain = jnp.clip(0.5 + 1.0 * jax.random.uniform(key_of[12], (HEADS,), jnp.float32) ** levels(key_of[12], (HEADS,), ((0, 8),), -0.2, 0.2), 0.5, 1.5)
    output_gain = jnp.clip(1.0 + 0.18 * jax.random.normal(key_of[13], (INNER,), jnp.float32), 0.1, 1.9)
    out_weight = noise(key_of[14], (INNER, WIDTH), INNER ** -0.5, 0.09375, ((0, 8), (1, 64)))
    base_state = noise(key_of[15], (SEQS, HEADS, HEAD_DIM, STATE_DIM), 0.3, 2.0, ((0, 64), (1, 8)), jnp.float32)
    past_value = noise(key_of[16], (SEQS, PAST_ROWS, INNER), 1.0, 6.0, ((0, 64), (2, 8)))
    past_write = noise(key_of[17], (SEQS, PAST_ROWS, GROUPS * STATE_DIM), 1.0, 6.0, ((0, 64), (2, 8)))
    past_read = noise(key_of[18], (SEQS, PAST_ROWS, GROUPS * STATE_DIM), 1.0, 6.0, ((0, 64), (2, 8)))
    past_step = noise(key_of[19], (SEQS, PROPOSALS, HEADS), 1.0, 4.0, ((0, 64), (2, 8)))
    accepted = plant(jax.random.randint(key_of[20], (SEQS,), 1, PROPOSALS + 1), jax.random.fold_in(key_of[20], 1), 1, PROPOSALS).astype(jnp.int32)
    return dict(tokens=tokens, input_gain=input_gain, gate_weight=gate_weight, value_weight=value_weight, write_weight=write_weight, read_weight=read_weight, step_weight=step_weight, conv_value=conv_value, conv_write=conv_write, conv_read=conv_read, step_bias=step_bias, decay_log=decay_log, skip_gain=skip_gain, output_gain=output_gain, out_weight=out_weight, base_state=base_state, past_value=past_value, past_write=past_write, past_read=past_read, past_step=past_step, accepted=accepted)


EPSILON = 1e-06

def causal_conv(rows, kernel):
    width = kernel.shape[0]
    count = rows.shape[0] - width + 1
    total = kernel[0] * rows[0:count]
    for offset in range(1, width):
        total = total + kernel[offset] * rows[offset:offset + count]
    return total

def advance(past_x, past_b, past_c, past_dt, taken, state_zero, value_now, write_now, read_now, gate_now, step_now, conv_value, conv_write, conv_read, step_bias, decay_log, skip_gain, output_gain):
    highest = lax.Precision.HIGHEST
    proposals = value_now.shape[0]
    head_count = step_bias.shape[0]
    group_count = write_now.shape[1] // STATE_DIM
    per_group = head_count // group_count
    head_width = value_now.shape[1] // head_count
    rate = jnp.exp(decay_log)
    taken = taken.astype(jnp.int32)
    prev_x = jax.nn.silu(causal_conv(past_x.astype(jnp.float32), conv_value)).reshape(proposals, head_count, head_width)
    prev_b = jax.nn.silu(causal_conv(past_b.astype(jnp.float32), conv_write)).reshape(proposals, group_count, STATE_DIM)
    prev_b = jnp.repeat(prev_b, per_group, axis=1)
    prev_dt = jax.nn.softplus(past_dt.astype(jnp.float32) + step_bias)
    live = (jnp.arange(proposals, dtype=jnp.int32) < taken)[:, None]
    prev_log = jnp.where(live, -rate * prev_dt, jnp.zeros_like(prev_dt))
    total_log = lax.optimization_barrier(jnp.sum(prev_log, axis=0))
    tail_log = total_log - jnp.cumsum(prev_log, axis=0)
    weight_now = jnp.where(live, jnp.exp(tail_log) * prev_dt, jnp.zeros_like(prev_dt))
    root = jnp.exp(total_log)[:, None, None] * state_zero + jnp.einsum('sh,shp,shn->hpn', weight_now, prev_x, prev_b, precision=highest)
    window_x = jnp.concatenate([lax.dynamic_slice_in_dim(past_x, taken, CONV_W - 1, 0), value_now], axis=0)
    window_b = jnp.concatenate([lax.dynamic_slice_in_dim(past_b, taken, CONV_W - 1, 0), write_now], axis=0)
    window_c = jnp.concatenate([lax.dynamic_slice_in_dim(past_c, taken, CONV_W - 1, 0), read_now], axis=0)
    cur_x = jax.nn.silu(causal_conv(window_x.astype(jnp.float32), conv_value)).reshape(proposals, head_count, head_width)
    cur_b = jax.nn.silu(causal_conv(window_b.astype(jnp.float32), conv_write)).reshape(proposals, group_count, STATE_DIM)
    cur_c = jax.nn.silu(causal_conv(window_c.astype(jnp.float32), conv_read)).reshape(proposals, group_count, STATE_DIM)
    cur_b = jnp.repeat(cur_b, per_group, axis=1)
    cur_c = jnp.repeat(cur_c, per_group, axis=1)
    cur_dt = jax.nn.softplus(step_now.astype(jnp.float32) + step_bias)
    logs = jnp.cumsum(-rate * cur_dt, axis=0)
    carried = jnp.einsum('thn,hpn->thp', cur_c, root, precision=highest) * jnp.exp(logs)[:, :, None]
    lower = (jnp.arange(proposals)[:, None] >= jnp.arange(proposals)[None, :])[:, :, None]
    diff = logs[:, None, :] - logs[None, :, :]
    decay = jnp.where(lower, jnp.exp(jnp.where(lower, diff, jnp.zeros_like(diff))), jnp.zeros_like(diff))
    scores = jnp.einsum('thn,shn->tsh', cur_c, cur_b, precision=highest) * decay * cur_dt[None, :, :]
    inner = jnp.einsum('tsh,shp->thp', scores, cur_x, precision=highest)
    mixed = carried + inner + skip_gain[None, :, None] * cur_x
    gated = mixed.reshape(proposals, -1) * jax.nn.silu(gate_now.astype(jnp.float32))
    grouped = gated.reshape(proposals, group_count, -1)
    grouped = grouped * lax.rsqrt(lax.optimization_barrier(jnp.mean(grouped * grouped, axis=-1, keepdims=True)) + EPSILON)
    result = (grouped.reshape(proposals, -1) * output_gain).astype(jnp.bfloat16)
    return (result, root, window_x, window_b, window_c)

def reference(tokens, input_gain, gate_weight, value_weight, write_weight, read_weight, step_weight, conv_value, conv_write, conv_read, step_bias, decay_log, skip_gain, output_gain, out_weight, base_state, past_value, past_write, past_read, past_step, accepted):
    seq_count, proposals, width = tokens.shape
    rows = tokens.astype(jnp.float32)
    normed = (rows * lax.rsqrt(lax.optimization_barrier(jnp.mean(rows * rows, axis=-1, keepdims=True)) + EPSILON) * input_gain).astype(jnp.bfloat16)
    flat = normed.reshape(seq_count * proposals, width)

    def project(weight):
        product = jnp.dot(flat, weight, preferred_element_type=jnp.float32).astype(jnp.bfloat16)
        return product.reshape(seq_count, proposals, weight.shape[1])
    gate_now = project(gate_weight)
    value_now = project(value_weight)
    write_now = project(write_weight)
    read_now = project(read_weight)
    step_now = project(step_weight)

    def one_sequence(items):
        return advance(*items, conv_value, conv_write, conv_read, step_bias, decay_log, skip_gain, output_gain)
    normal_out, root_state, next_value, next_write, next_read = lax.map(one_sequence, (past_value, past_write, past_read, past_step, accepted, base_state, value_now, write_now, read_now, gate_now, step_now))
    flat_y = normal_out.reshape(seq_count * proposals, -1)
    block = flat_y.shape[1] // N_TP
    total = jnp.zeros((seq_count * proposals, width), jnp.float32)
    for portion in range(N_TP):
        partial_sum = jnp.dot(flat_y[:, portion * block:(portion + 1) * block], out_weight[portion * block:(portion + 1) * block], preferred_element_type=jnp.float32)
        total = total + lax.optimization_barrier(partial_sum.astype(jnp.bfloat16)).astype(jnp.float32)
    mixed = total.astype(jnp.bfloat16).reshape(seq_count, proposals, width)
    return (mixed, root_state, next_value, next_write, next_read, step_now)
```

```python
import jax
import jax.numpy as jnp
from jax import lax
from jax.experimental import pallas as pl
from jax.experimental.pallas import tpu as pltpu
from jax.sharding import PartitionSpec as P

F32 = jnp.float32
BF16 = jnp.bfloat16
MESH = pl.DeviceIdType.MESH
EPSILON = 1e-06
HIGHEST = lax.Precision.HIGHEST

N = 8
SEQ = 4
PROP = 4
ROWS = SEQ * PROP
CONV = 4
PAST = 7
NT = (((1,), (1,)), ((), ()))
TN = (((0,), (0,)), ((), ()))
FAR = (4, 3, 5)
NEAR = (2, 6, 1, 7)

T1, T2Y, T2Z, WY, WZ, RSY, RSZ, OW, O1, O2 = range(10)


def silu(v):
    return v / (1.0 + jnp.exp(-v))


def softplus(v):
    return jnp.maximum(v, 0.0) + jnp.log1p(jnp.exp(-jnp.abs(v)))


def conv(buf, taps, at=0):
    total = taps[0:1, :] * buf[at : at + ROWS, :]
    for k in range(1, CONV):
        total = total + taps[k : k + 1, :] * buf[at + SEQ * k : at + SEQ * k + ROWS, :]
    return total


def body(
    tokens, input_gain, gate_w, value_w, write_w, read_w, step_w,
    conv_v, conv_b, conv_c, step_bias, decay_log, skip_gain, output_gain,
    out_w, base, past_v, past_b, past_c, past_s, accepted,
    mixed_o, root_o, nv_o, nb_o, nc_o, ns_o,
    gain_m, stepw_m, cv_m, cb_m, cc_m, bias_m, decay_m, skip_m, og_m,
    base_m, pv_m, pb_m, pc_m, ps_m,
    xall, nrm, npk, ay, az, wy, wz, py, pz, rsy, rsz, owg, nrg, po, osum,
    xf, ppv, ppb, ppc, rrv, rrb, rrc, stp, sbuf, ubuf, bbuf, xb, bb, lb, dtb, dj, rootb, mf, nsf,
    mixed_m, root_m, nv_m, nb_m, nc_m, ns_m,
    in_sem, out_sem, send_sem, recv_sem,
):
    kv = lax.axis_index("kv")
    tp = lax.axis_index("tp")
    z = kv // N
    y = kv % N

    def at(rows, count):
        return pl.ds(pl.multiple_of(rows * count, count), count)

    ins = [
        (value_w, wy.at[at(y, 32), pl.ds(0, 512)]),
        (write_w, wy.at[at(y, 32), pl.ds(512, 128)]),
        (gate_w, wz.at[at(z, 32), pl.ds(0, 512)]),
        (read_w, wz.at[at(z, 32), pl.ds(512, 128)]),
        (out_w, owg.at[at(y, 32), :]),
        (tokens, xall.at[tp]),
        (input_gain, gain_m),
        (past_v, pv_m),
        (past_b, pb_m),
        (past_c, pc_m),
        (past_s, ps_m),
        (conv_v, cv_m),
        (conv_b, cb_m),
        (conv_c, cc_m),
        (step_bias, bias_m),
        (decay_log, decay_m),
        (skip_gain, skip_m),
        (output_gain, og_m),
        (step_w, stepw_m),
        (base, base_m),
    ]
    loads = [pltpu.make_async_copy(s, d, in_sem.at[i]) for i, (s, d) in enumerate(ins)]
    for c in loads:
        c.start()

    barrier = pltpu.get_barrier_semaphore()

    def tell(k, t):
        pl.semaphore_signal(barrier, inc=1, device_id=(k, t), device_id_type=MESH)

    for d in range(1, N):
        tell(kv, (tp + d) % N)
        tell(z * N + (y + d) % N, tp)
        tell(((z + d) % N) * N + y, tp)
        tell(tp * N + y, (tp + d) % N)

    @pl.when(z != tp)
    def _():
        tell(tp * N + y, tp)

    for c in loads[:6]:
        c.wait()
    pl.semaphore_wait(barrier, 4 * (N - 1) + jnp.where(z != tp, 1, 0).astype(jnp.int32))

    sent = []

    def send(phase, d, src, dst, slot, k, t):
        c = pltpu.make_async_remote_copy(
            src_ref=src, dst_ref=dst, send_sem=send_sem.at[phase, d],
            recv_sem=recv_sem.at[phase, slot], device_id=(k, t), device_id_type=MESH,
        )
        c.start()
        sent.append(c)

    def arrived(phase, slot, ref):
        pltpu.make_async_remote_copy(
            src_ref=ref, dst_ref=ref, send_sem=send_sem.at[phase, 0],
            recv_sem=recv_sem.at[phase, slot], device_id=(kv, tp), device_id_type=MESH,
        ).wait_recv()

    def up(d):
        return z * N + (y + d) % N

    def over(d):
        return ((z + d) % N) * N + y

    def weights(ds):
        for d in ds:
            send(WY, d, wy.at[at(y, 32), :], wy.at[at(y, 32), :], y, up(d), tp)
            send(WZ, d, wz.at[at(z, 32), :], wz.at[at(z, 32), :], z, over(d), tp)

    for d in range(1, N):
        send(T1, d, xall.at[tp], xall.at[tp], tp, kv, (tp + d) % N)
    weights(FAR)

    for c in loads[6:]:
        c.wait()
    for r in range(PAST):
        ppv[SEQ * r : SEQ * r + SEQ, :] = pv_m[r].astype(F32)
        ppb[SEQ * r : SEQ * r + SEQ, :] = pb_m[r].astype(F32)
        ppc[SEQ * r : SEQ * r + SEQ, :] = pc_m[r].astype(F32)

    for d in range(1, N):
        t = (tp + d) % N
        arrived(T1, t, xall.at[t])
    for t in range(N):
        for q in range(SEQ):
            xf[PROP * q : PROP * q + PROP, 256 * t : 256 * t + 256] = xall[t, q].astype(F32)
    rows = xf[...]
    scale = lax.rsqrt(jnp.mean(rows * rows, axis=-1, keepdims=True) + EPSILON)
    normed16 = (rows * scale * gain_m[...]).astype(BF16)
    to = lax.broadcasted_iota(jnp.int32, (ROWS, ROWS), 0)
    by = lax.broadcasted_iota(jnp.int32, (ROWS, ROWS), 1)
    swap = jnp.where((to % SEQ) * PROP + to // SEQ == by, 1.0, 0.0).astype(BF16)
    normed = jnp.dot(swap, normed16, preferred_element_type=F32)
    normed16 = normed.astype(BF16)
    for zz in range(N):
        nrm[zz] = normed16[:, 256 * zz : 256 * zz + 256]
    lane = lax.broadcasted_iota(jnp.int32, (ROWS, 128), 1) // 32
    for yy in range(N):
        for half in range(2):
            tile = None
            for i in range(4):
                start = 256 * (4 * half + i) + 128 * (yy // 4)
                shift = (32 * i - 32 * (yy % 4)) % 128
                piece = normed[:, start : start + 128]
                if shift:
                    piece = pltpu.roll(piece, shift, 1)
                tile = piece if tile is None else jnp.where(lane == i, piece, tile)
            npk[yy, :, 128 * half : 128 * half + 128] = tile.astype(BF16)
    ay[at(z, ROWS), :] = nrm[z]
    az[at(y, ROWS), :] = npk[y]
    for d in FAR + NEAR:
        zz, yy = (z + d) % N, (y + d) % N
        send(T2Y, d, nrm.at[zz], ay.at[at(z, ROWS), :], z, over(d), tp)
        send(T2Z, d, npk.at[yy], az.at[at(y, ROWS), :], y, up(d), tp)
    weights(NEAR)

    head = lax.broadcasted_iota(jnp.int32, (1, 512), 1) // 64

    def spread(ref):
        row = jnp.zeros((1, 512), F32)
        for h in range(8):
            row = jnp.where(head == h, ref[0:1, h : h + 1], row)
        return row

    bias = spread(bias_m)
    rate = jnp.exp(spread(decay_m))
    skip = spread(skip_m)
    step16 = lax.dot_general(normed16, stepw_m[...], NT, preferred_element_type=F32).astype(BF16)
    row64 = lax.broadcasted_iota(jnp.int32, (64, 512), 0)
    own64 = (row64 - 8 * tp == lax.broadcasted_iota(jnp.int32, (64, 512), 1) // 64)
    wide = jnp.dot(step16, jnp.where(own64, 1.0, 0.0).astype(BF16), preferred_element_type=F32)
    row64 = lax.broadcasted_iota(jnp.int32, (64, 128), 0)
    pick = (row64 - 8 * tp == lax.broadcasted_iota(jnp.int32, (64, 128), 1))
    nsf[...] = jnp.dot(step16, jnp.where(pick, 1.0, 0.0).astype(BF16), preferred_element_type=F32)
    for q in range(SEQ):
        ns_m[q] = nsf[pl.ds(q, PROP, stride=SEQ), :][:, 0:8].astype(BF16)

    dt = softplus(wide + bias)
    sbuf[...] = -rate * dt
    run = jnp.zeros((SEQ, 512), F32)
    lb[0:12, :] = jnp.zeros((12, 512), F32)
    dtb[0:12, :] = jnp.zeros((12, 512), F32)
    xb[0:12, :] = jnp.zeros((12, 512), F32)
    bb[0:12, :] = jnp.zeros((12, 128), F32)
    for t in range(PROP):
        run = run + sbuf[SEQ * t : SEQ * t + SEQ, :]
        lb[12 + SEQ * t : 16 + SEQ * t, :] = run
    dtb[12:28, :] = dt
    logs = lb[12:28, :]
    for j in range(PROP):
        lo = 12 - SEQ * j
        dj[j] = jnp.exp(logs - lb[lo : lo + ROWS, :]) * dtb[lo : lo + ROWS, :]

    eight = (
        lax.broadcasted_iota(jnp.int32, (8, 512), 0)
        == lax.broadcasted_iota(jnp.int32, (8, 512), 1) // 64
    )
    eight = jnp.where(eight, 1.0, 0.0).astype(BF16)
    for q in range(SEQ):
        stp[PROP * q : PROP * q + PROP, :] = jnp.dot(
            ps_m[q], eight, preferred_element_type=F32
        )
    steps = jnp.dot(swap, stp[...].astype(BF16), preferred_element_type=F32)
    pd = softplus(steps + bias)

    def taken(shape):
        seq = lax.broadcasted_iota(jnp.int32, shape, 0) % SEQ
        count = jnp.full(shape, accepted[0], jnp.int32)
        for q in range(1, SEQ):
            count = jnp.where(seq == q, accepted[q], count)
        return count

    live = lax.broadcasted_iota(jnp.int32, (ROWS, 512), 0) // SEQ < taken((ROWS, 512))
    sbuf[...] = jnp.where(live, -rate * pd, 0.0)
    pls = [sbuf[SEQ * s : SEQ * s + SEQ, :] for s in range(PROP)]
    tails = [None] * PROP
    run = jnp.zeros((SEQ, 512), F32)
    for s in reversed(range(PROP)):
        tails[s] = run
        run = run + pls[s]
    kept = jnp.exp(run)
    for s in range(PROP):
        stp[SEQ * s : SEQ * s + SEQ, :] = jnp.exp(tails[s])
    ubuf[...] = jnp.where(live, stp[...] * pd, 0.0) * silu(conv(ppv, cv_m))
    bbuf[...] = silu(conv(ppb, cb_m))

    def window(pp, rr, width):
        count = taken((12, width))
        first = pp[SEQ : SEQ + 12, :]
        for a in range(2, PROP + 1):
            first = jnp.where(count == a, pp[SEQ * a : SEQ * a + 12, :], first)
        rr[0:12, :] = first

    window(ppv, rrv, 512)
    window(ppb, rrb, 128)
    window(ppc, rrc, 128)

    for d in range(1, N):
        zz, yy = (z + d) % N, (y + d) % N
        arrived(T2Y, zz, ay.at[at(zz, ROWS), :])
        arrived(T2Z, yy, az.at[at(yy, ROWS), :])
    for d in FAR + NEAR:
        yy = (y + d) % N
        arrived(WY, yy, wy.at[at(yy, 32), :])
    py[...] = jnp.dot(ay[...], wy[...], preferred_element_type=F32).astype(BF16)
    for d in FAR + NEAR:
        zz = (z + d) % N
        arrived(WZ, zz, wz.at[at(zz, 32), :])
    pz[...] = jnp.dot(az[...], wz[...], preferred_element_type=F32).astype(BF16)
    for d in FAR + NEAR:
        zz, yy = (z + d) % N, (y + d) % N
        send(RSY, d, py.at[at(zz, ROWS), :], rsy.at[z], z, over(d), tp)
        send(RSZ, d, pz.at[at(yy, ROWS), :], rsz.at[y], y, up(d), tp)
    for d in FAR + NEAR:
        send(OW, d, owg.at[at(y, 32), :], owg.at[at(y, 32), :], y, up(d), tp)
    rsy[z] = py[at(z, ROWS), :]
    rsz[y] = pz[at(y, ROWS), :]

    seq = lax.broadcasted_iota(jnp.int32, (ROWS, 512), 0) % SEQ
    for q in range(SEQ):
        u = jnp.where(seq == q, ubuf[...], 0.0)
        grown = lax.dot_general(u, bbuf[...], TN, precision=HIGHEST, preferred_element_type=F32)
        for h in range(8):
            lo = 512 * q + 64 * h
            old = jnp.broadcast_to(kept[q : q + 1, 64 * h : 64 * h + 1], (64, 128))
            new = old * base_m[lo : lo + 64, :] + grown[64 * h : 64 * h + 64, :]
            root_m[lo : lo + 64, :] = new
            rootb[lo : lo + 64, :] = new.astype(BF16)

    outs = []

    def put(src, dst):
        c = pltpu.make_async_copy(src, dst, out_sem.at[len(outs)])
        c.start()
        outs.append(c)

    put(root_m, root_o)
    put(ns_m, ns_o)

    for d in FAR + NEAR:
        zz, yy = (z + d) % N, (y + d) % N
        arrived(RSY, zz, rsy.at[zz])
        arrived(RSZ, yy, rsz.at[yy])

    def summed(ref, lo, hi):
        total = ref[0, :, lo:hi].astype(F32)
        for s in range(1, N):
            total = total + ref[s, :, lo:hi].astype(F32)
        return total.astype(BF16).astype(F32)

    rrv[12:28, :] = summed(rsy, 0, 512)
    rrb[12:28, :] = summed(rsy, 512, 640)
    rrc[12:28, :] = summed(rsz, 512, 640)
    gate = summed(rsz, 0, 512)
    x = silu(conv(rrv, cv_m))
    b = silu(conv(rrb, cb_m))
    c = silu(conv(rrc, cc_m))
    xb[12:28, :] = x
    bb[12:28, :] = b
    c16 = c.astype(BF16)
    carried = jnp.zeros((ROWS, 512), F32)
    for q in range(SEQ):
        one = lax.dot_general(
            c16, rootb[512 * q : 512 * q + 512, :], NT, preferred_element_type=F32
        )
        carried = jnp.where(seq == q, one, carried)
    out = jnp.exp(logs) * carried + skip * x
    for j in range(PROP):
        lo = 12 - SEQ * j
        score = jnp.sum(c * bb[lo : lo + ROWS, :], axis=-1, keepdims=True)
        out = out + score * dj[j] * xb[lo : lo + ROWS, :]
    g = out * silu(gate)
    g = g * lax.rsqrt(jnp.mean(g * g, axis=-1, keepdims=True) + EPSILON)
    nrg[at(z, ROWS), :] = (g * og_m[...]).astype(BF16)
    for d in FAR + NEAR:
        send(O1, d, nrg.at[at(z, ROWS), :], nrg.at[at(z, ROWS), :], z, over(d), tp)

    for r in range(PAST):
        nv_m[r] = rrv[SEQ * r : SEQ * r + SEQ, :].astype(BF16)
        nb_m[r] = rrb[SEQ * r : SEQ * r + SEQ, :].astype(BF16)
        nc_m[r] = rrc[SEQ * r : SEQ * r + SEQ, :].astype(BF16)
    put(nv_m, nv_o)
    put(nb_m, nb_o)
    put(nc_m, nc_o)

    for d in FAR + NEAR:
        yy = (y + d) % N
        arrived(OW, yy, owg.at[at(yy, 32), :])
    for d in FAR + NEAR:
        zz = (z + d) % N
        arrived(O1, zz, nrg.at[at(zz, ROWS), :])
    po[...] = lax.dot_general(nrg[...], owg[...], NT, preferred_element_type=F32).astype(BF16)

    def back(d):
        zz = (z + d) % N
        return pltpu.make_async_remote_copy(
            src_ref=po.at[at(zz, ROWS), :], dst_ref=osum.at[tp], send_sem=send_sem.at[O2, d],
            recv_sem=recv_sem.at[O2, tp], device_id=(over(d), z), device_id_type=MESH,
        )

    for d in FAR + NEAR:
        back(d).start()

    @pl.when(z != tp)
    def _():
        back(0).start()

    @pl.when(z == tp)
    def _():
        osum[tp] = po[at(z, ROWS), :]

    for d in range(1, N):
        t = (tp + d) % N
        arrived(O2, t, osum.at[t])

    @pl.when(z != tp)
    def _():
        arrived(O2, tp, osum.at[tp])

    total = osum[0].astype(F32)
    for t in range(1, N):
        total = total + osum[t].astype(F32)
    for i in range(2):
        mf[i] = total[:, 128 * i : 128 * i + 128]
        for q in range(SEQ):
            mixed_m[q, :, 128 * i : 128 * i + 128] = mf.at[i][
                pl.ds(q, PROP, stride=SEQ), :
            ].astype(BF16)
    put(mixed_m, mixed_o)

    for c in sent:
        c.wait_send()
    for d in range(1, N):
        back(d).wait_send()

    @pl.when(z != tp)
    def _():
        back(0).wait_send()

    for c in outs:
        c.wait()


def on_device(
    tokens, input_gain, gate_weight, value_weight, write_weight, read_weight, step_weight,
    conv_value, conv_write, conv_read, step_bias, decay_log, skip_gain, output_gain,
    out_weight, base_state, past_value, past_write, past_read, past_step, accepted,
):
    vmem = pltpu.VMEM
    ops = (
        tokens, input_gain[None, :], gate_weight, value_weight, write_weight, read_weight,
        step_weight.T, conv_value, conv_write, conv_read, step_bias[None, :],
        decay_log[None, :], skip_gain[None, :], output_gain[None, :], out_weight.T,
        base_state.reshape(2048, 128), past_value.transpose(1, 0, 2),
        past_write.transpose(1, 0, 2), past_read.transpose(1, 0, 2), past_step, accepted,
    )
    out_shapes = [
        ((SEQ, PROP, 256), BF16), ((2048, 128), F32), ((PAST, SEQ, 512), BF16),
        ((PAST, SEQ, 128), BF16), ((PAST, SEQ, 128), BF16), ((SEQ, PROP, 8), BF16),
    ]
    scratch = [
        vmem((1, 2048), F32), vmem((64, 2048), BF16), vmem((4, 512), F32), vmem((4, 128), F32),
        vmem((4, 128), F32), vmem((1, 8), F32), vmem((1, 8), F32), vmem((1, 8), F32),
        vmem((1, 512), F32), vmem((2048, 128), F32), vmem((PAST, SEQ, 512), BF16),
        vmem((PAST, SEQ, 128), BF16), vmem((PAST, SEQ, 128), BF16), vmem((SEQ, PROP, 8), BF16),
        vmem((N, SEQ, PROP, 256), BF16), vmem((N, ROWS, 256), BF16), vmem((N, ROWS, 256), BF16),
        vmem((128, 256), BF16), vmem((128, 256), BF16), vmem((256, 640), BF16),
        vmem((256, 640), BF16), vmem((128, 640), BF16), vmem((128, 640), BF16),
        vmem((N, ROWS, 640), BF16), vmem((N, ROWS, 640), BF16), vmem((256, 512), BF16),
        vmem((128, 512), BF16), vmem((128, 256), BF16), vmem((N, ROWS, 256), BF16),
        vmem((ROWS, 2048), F32), vmem((28, 512), F32), vmem((28, 128), F32), vmem((28, 128), F32),
        vmem((28, 512), F32), vmem((28, 128), F32), vmem((28, 128), F32), vmem((ROWS, 512), F32),
        vmem((ROWS, 512), F32), vmem((ROWS, 512), F32), vmem((ROWS, 128), F32),
        vmem((28, 512), F32), vmem((28, 128), F32), vmem((28, 512), F32), vmem((28, 512), F32),
        vmem((PROP, ROWS, 512), F32), vmem((2048, 128), BF16), vmem((2, ROWS, 128), F32),
        vmem((ROWS, 128), F32),
        *(vmem(shape, dtype) for shape, dtype in out_shapes),
        pltpu.SemaphoreType.DMA((20,)),
        pltpu.SemaphoreType.DMA((6,)),
        pltpu.SemaphoreType.DMA((10, N)),
        pltpu.SemaphoreType.DMA((10, N)),
    ]
    mixed, root, nv, nb, nc, ns = pl.pallas_call(
        body,
        out_shape=[jax.ShapeDtypeStruct(shape, dtype) for shape, dtype in out_shapes],
        in_specs=[pl.BlockSpec(memory_space=pl.ANY)] * 20
        + [pl.BlockSpec(memory_space=pltpu.SMEM)],
        out_specs=[pl.BlockSpec(memory_space=pl.ANY)] * 6,
        scratch_shapes=scratch,
        compiler_params=pltpu.CompilerParams(collective_id=0, has_side_effects=True),
        name="mixer",
    )(*ops)
    return (
        mixed, root.reshape(base_state.shape), nv.transpose(1, 0, 2), nb.transpose(1, 0, 2),
        nc.transpose(1, 0, 2), ns,
    )


def solution(mesh):
    return jax.shard_map(
        on_device,
        mesh=mesh,
        in_specs=(
            P("kv", None, "tp"), P(), P("kv", "tp"), P("kv", "tp"), P("kv", "tp"), P("kv", "tp"),
            P(), P(None, "tp"), P(None, "tp"), P(None, "tp"), P("tp"), P("tp"), P("tp"), P("tp"),
            P("tp", "kv"), P("kv", "tp", None, None), P("kv", None, "tp"), P("kv", None, "tp"),
            P("kv", None, "tp"), P("kv", None, "tp"), P("kv"),
        ),
        out_specs=(
            P("kv", None, "tp"), P("kv", "tp", None, None), P("kv", None, "tp"),
            P("kv", None, "tp"), P("kv", None, "tp"), P("kv", None, "tp"),
        ),
        check_vma=False,
    )
```

```python
import jax
import jax.numpy as jnp
from jax import lax
from jax.experimental import pallas as pl
from jax.experimental.pallas import tpu as pltpu
from jax.sharding import PartitionSpec as P

F32 = jnp.float32
BF16 = jnp.bfloat16
MESH = pl.DeviceIdType.MESH
EPSILON = 1e-06
HIGHEST = lax.Precision.HIGHEST

N = 8
SEQ = 4
PROP = 4
ROWS = SEQ * PROP
CONV = 4
PAST = 7
NT = (((1,), (1,)), ((), ()))
TN = (((0,), (0,)), ((), ()))
FAR = (4, 3, 5)
NEAR = (2, 6, 1, 7)

T1, T2Y, T2Z, WY, WZ, RSY, RSZ, OW, O1, O2 = range(10)


def silu(v):
    return v / (1.0 + jnp.exp(-v))


def softplus(v):
    return jnp.maximum(v, 0.0) + jnp.log1p(jnp.exp(-jnp.abs(v)))


def conv(buf, taps, at=0):
    total = taps[0:1, :] * buf[at : at + ROWS, :]
    for k in range(1, CONV):
        total = total + taps[k : k + 1, :] * buf[at + SEQ * k : at + SEQ * k + ROWS, :]
    return total


def body(
    tokens, input_gain, gate_w, value_w, write_w, read_w, step_w,
    conv_v, conv_b, conv_c, step_bias, decay_log, skip_gain, output_gain,
    out_w, base, past_v, past_b, past_c, past_s, accepted,
    mixed_m, root_m, nv_m, nb_m, nc_m, ns_m,
    gain_m, stepw_m, cv_m, cb_m, cc_m, bias_m, decay_m, skip_m, og_m,
    base_m, pv_m, pb_m, pc_m, ps_m,
    xall, nrm, npk, ay, az, wy, wz, py, pz, rsy, rsz, owg, nrg, po, osum,
    xf, ppv, ppb, ppc, rrv, rrb, rrc, stp, sbuf, ubuf, bbuf, xb, bb, lb, dtb, dj, rootb, mf, nsf,
    taken_m,
    in_sem, send_sem, recv_sem,
):
    kv = lax.axis_index("kv")
    tp = lax.axis_index("tp")
    z = kv // N
    y = kv % N

    def at(rows, count):
        return pl.ds(pl.multiple_of(rows * count, count), count)

    ins = [
        (value_w, wy.at[at(y, 32), pl.ds(0, 512)]),
        (write_w, wy.at[at(y, 32), pl.ds(512, 128)]),
        (gate_w, wz.at[at(z, 32), pl.ds(0, 512)]),
        (read_w, wz.at[at(z, 32), pl.ds(512, 128)]),
        (out_w, owg.at[at(y, 32), :]),
        (tokens, xall.at[tp]),
        (input_gain, gain_m),
        (past_v, pv_m),
        (past_b, pb_m),
        (past_c, pc_m),
        (past_s, ps_m),
        (conv_v, cv_m),
        (conv_b, cb_m),
        (conv_c, cc_m),
        (step_bias, bias_m),
        (decay_log, decay_m),
        (skip_gain, skip_m),
        (output_gain, og_m),
        (step_w, stepw_m),
        (base, base_m),
        (accepted, taken_m),
    ]
    loads = [pltpu.make_async_copy(s, d, in_sem.at[i]) for i, (s, d) in enumerate(ins)]
    for c in loads:
        c.start()

    barrier = pltpu.get_barrier_semaphore()

    def tell(k, t):
        pl.semaphore_signal(barrier, inc=1, device_id=(k, t), device_id_type=MESH)

    for d in range(1, N):
        tell(kv, (tp + d) % N)
        tell(z * N + (y + d) % N, tp)
        tell(((z + d) % N) * N + y, tp)
        tell(tp * N + y, (tp + d) % N)

    @pl.when(z != tp)
    def _():
        tell(tp * N + y, tp)

    for c in loads[:6]:
        c.wait()
    pl.semaphore_wait(barrier, 4 * (N - 1) + jnp.where(z != tp, 1, 0).astype(jnp.int32))

    sent = []

    def send(phase, d, src, dst, slot, k, t):
        c = pltpu.make_async_remote_copy(
            src_ref=src, dst_ref=dst, send_sem=send_sem.at[phase, d],
            recv_sem=recv_sem.at[phase, slot], device_id=(k, t), device_id_type=MESH,
        )
        c.start()
        sent.append(c)

    def arrived(phase, slot, ref):
        pltpu.make_async_remote_copy(
            src_ref=ref, dst_ref=ref, send_sem=send_sem.at[phase, 0],
            recv_sem=recv_sem.at[phase, slot], device_id=(kv, tp), device_id_type=MESH,
        ).wait_recv()

    def up(d):
        return z * N + (y + d) % N

    def over(d):
        return ((z + d) % N) * N + y

    def weights(ds):
        for d in ds:
            send(WY, d, wy.at[at(y, 32), :], wy.at[at(y, 32), :], y, up(d), tp)
            send(WZ, d, wz.at[at(z, 32), :], wz.at[at(z, 32), :], z, over(d), tp)

    for d in range(1, N):
        send(T1, d, xall.at[tp], xall.at[tp], tp, kv, (tp + d) % N)
    weights(FAR)

    for c in loads[6:]:
        c.wait()
    for r in range(PAST):
        ppv[SEQ * r : SEQ * r + SEQ, :] = pv_m[r].astype(F32)
        ppb[SEQ * r : SEQ * r + SEQ, :] = pb_m[r].astype(F32)
        ppc[SEQ * r : SEQ * r + SEQ, :] = pc_m[r].astype(F32)

    for d in range(1, N):
        t = (tp + d) % N
        arrived(T1, t, xall.at[t])
    for t in range(N):
        for q in range(SEQ):
            xf[PROP * q : PROP * q + PROP, 256 * t : 256 * t + 256] = xall[t, q].astype(F32)
    rows = xf[...]
    scale = lax.rsqrt(jnp.mean(rows * rows, axis=-1, keepdims=True) + EPSILON)
    normed16 = (rows * scale * gain_m[...]).astype(BF16)
    to = lax.broadcasted_iota(jnp.int32, (ROWS, ROWS), 0)
    by = lax.broadcasted_iota(jnp.int32, (ROWS, ROWS), 1)
    swap = jnp.where((to % SEQ) * PROP + to // SEQ == by, 1.0, 0.0).astype(BF16)
    normed = jnp.dot(swap, normed16, preferred_element_type=F32)
    normed16 = normed.astype(BF16)
    for zz in range(N):
        nrm[zz] = normed16[:, 256 * zz : 256 * zz + 256]
    lane = lax.broadcasted_iota(jnp.int32, (ROWS, 128), 1) // 32
    for yy in range(N):
        for half in range(2):
            tile = None
            for i in range(4):
                start = 256 * (4 * half + i) + 128 * (yy // 4)
                shift = (32 * i - 32 * (yy % 4)) % 128
                piece = normed[:, start : start + 128]
                if shift:
                    piece = pltpu.roll(piece, shift, 1)
                tile = piece if tile is None else jnp.where(lane == i, piece, tile)
            npk[yy, :, 128 * half : 128 * half + 128] = tile.astype(BF16)
    ay[at(z, ROWS), :] = nrm[z]
    az[at(y, ROWS), :] = npk[y]
    for d in FAR + NEAR:
        zz, yy = (z + d) % N, (y + d) % N
        send(T2Y, d, nrm.at[zz], ay.at[at(z, ROWS), :], z, over(d), tp)
        send(T2Z, d, npk.at[yy], az.at[at(y, ROWS), :], y, up(d), tp)
    weights(NEAR)

    head = lax.broadcasted_iota(jnp.int32, (1, 512), 1) // 64

    def spread(ref):
        row = jnp.zeros((1, 512), F32)
        for h in range(8):
            row = jnp.where(head == h, ref[0:1, h : h + 1], row)
        return row

    bias = spread(bias_m)
    rate = jnp.exp(spread(decay_m))
    skip = spread(skip_m)
    step16 = lax.dot_general(normed16, stepw_m[...], NT, preferred_element_type=F32).astype(BF16)
    row64 = lax.broadcasted_iota(jnp.int32, (64, 512), 0)
    own64 = (row64 - 8 * tp == lax.broadcasted_iota(jnp.int32, (64, 512), 1) // 64)
    wide = jnp.dot(step16, jnp.where(own64, 1.0, 0.0).astype(BF16), preferred_element_type=F32)
    row64 = lax.broadcasted_iota(jnp.int32, (64, 128), 0)
    pick = (row64 - 8 * tp == lax.broadcasted_iota(jnp.int32, (64, 128), 1))
    nsf[...] = jnp.dot(step16, jnp.where(pick, 1.0, 0.0).astype(BF16), preferred_element_type=F32)
    for q in range(SEQ):
        ns_m[q] = nsf[pl.ds(q, PROP, stride=SEQ), :][:, 0:8].astype(BF16)

    dt = softplus(wide + bias)
    sbuf[...] = -rate * dt
    run = jnp.zeros((SEQ, 512), F32)
    lb[0:12, :] = jnp.zeros((12, 512), F32)
    dtb[0:12, :] = jnp.zeros((12, 512), F32)
    xb[0:12, :] = jnp.zeros((12, 512), F32)
    bb[0:12, :] = jnp.zeros((12, 128), F32)
    for t in range(PROP):
        run = run + sbuf[SEQ * t : SEQ * t + SEQ, :]
        lb[12 + SEQ * t : 16 + SEQ * t, :] = run
    dtb[12:28, :] = dt
    logs = lb[12:28, :]
    for j in range(PROP):
        lo = 12 - SEQ * j
        dj[j] = jnp.exp(logs - lb[lo : lo + ROWS, :]) * dtb[lo : lo + ROWS, :]

    eight = (
        lax.broadcasted_iota(jnp.int32, (8, 512), 0)
        == lax.broadcasted_iota(jnp.int32, (8, 512), 1) // 64
    )
    eight = jnp.where(eight, 1.0, 0.0).astype(BF16)
    for q in range(SEQ):
        stp[PROP * q : PROP * q + PROP, :] = jnp.dot(
            ps_m[q], eight, preferred_element_type=F32
        )
    steps = jnp.dot(swap, stp[...].astype(BF16), preferred_element_type=F32)
    pd = softplus(steps + bias)

    def taken(shape):
        seq = lax.broadcasted_iota(jnp.int32, shape, 0) % SEQ
        count = jnp.full(shape, taken_m[0], jnp.int32)
        for q in range(1, SEQ):
            count = jnp.where(seq == q, taken_m[q], count)
        return count

    live = lax.broadcasted_iota(jnp.int32, (ROWS, 512), 0) // SEQ < taken((ROWS, 512))
    sbuf[...] = jnp.where(live, -rate * pd, 0.0)
    pls = [sbuf[SEQ * s : SEQ * s + SEQ, :] for s in range(PROP)]
    tails = [None] * PROP
    run = jnp.zeros((SEQ, 512), F32)
    for s in reversed(range(PROP)):
        tails[s] = run
        run = run + pls[s]
    kept = jnp.exp(run)
    for s in range(PROP):
        stp[SEQ * s : SEQ * s + SEQ, :] = jnp.exp(tails[s])
    ubuf[...] = jnp.where(live, stp[...] * pd, 0.0) * silu(conv(ppv, cv_m))
    bbuf[...] = silu(conv(ppb, cb_m))

    def window(pp, rr, width):
        count = taken((12, width))
        first = pp[SEQ : SEQ + 12, :]
        for a in range(2, PROP + 1):
            first = jnp.where(count == a, pp[SEQ * a : SEQ * a + 12, :], first)
        rr[0:12, :] = first

    window(ppv, rrv, 512)
    window(ppb, rrb, 128)
    window(ppc, rrc, 128)

    for d in range(1, N):
        zz, yy = (z + d) % N, (y + d) % N
        arrived(T2Y, zz, ay.at[at(zz, ROWS), :])
        arrived(T2Z, yy, az.at[at(yy, ROWS), :])
    for d in FAR + NEAR:
        yy = (y + d) % N
        arrived(WY, yy, wy.at[at(yy, 32), :])
    py[...] = jnp.dot(ay[...], wy[...], preferred_element_type=F32).astype(BF16)
    for d in FAR + NEAR:
        zz = (z + d) % N
        arrived(WZ, zz, wz.at[at(zz, 32), :])
    pz[...] = jnp.dot(az[...], wz[...], preferred_element_type=F32).astype(BF16)
    for d in FAR + NEAR:
        zz, yy = (z + d) % N, (y + d) % N
        send(RSY, d, py.at[at(zz, ROWS), :], rsy.at[z], z, over(d), tp)
        send(RSZ, d, pz.at[at(yy, ROWS), :], rsz.at[y], y, up(d), tp)
    for d in FAR + NEAR:
        send(OW, d, owg.at[at(y, 32), :], owg.at[at(y, 32), :], y, up(d), tp)
    rsy[z] = py[at(z, ROWS), :]
    rsz[y] = pz[at(y, ROWS), :]

    seq = lax.broadcasted_iota(jnp.int32, (ROWS, 512), 0) % SEQ
    for q in range(SEQ):
        u = jnp.where(seq == q, ubuf[...], 0.0)
        grown = lax.dot_general(u, bbuf[...], TN, precision=HIGHEST, preferred_element_type=F32)
        for h in range(8):
            lo = 512 * q + 64 * h
            old = jnp.broadcast_to(kept[q : q + 1, 64 * h : 64 * h + 1], (64, 128))
            new = old * base_m[lo : lo + 64, :] + grown[64 * h : 64 * h + 64, :]
            root_m[lo : lo + 64, :] = new
            rootb[lo : lo + 64, :] = new.astype(BF16)

    for d in FAR + NEAR:
        zz, yy = (z + d) % N, (y + d) % N
        arrived(RSY, zz, rsy.at[zz])
        arrived(RSZ, yy, rsz.at[yy])

    def summed(ref, lo, hi):
        total = ref[0, :, lo:hi].astype(F32)
        for s in range(1, N):
            total = total + ref[s, :, lo:hi].astype(F32)
        return total.astype(BF16).astype(F32)

    rrv[12:28, :] = summed(rsy, 0, 512)
    rrb[12:28, :] = summed(rsy, 512, 640)
    rrc[12:28, :] = summed(rsz, 512, 640)
    gate = summed(rsz, 0, 512)
    x = silu(conv(rrv, cv_m))
    b = silu(conv(rrb, cb_m))
    c = silu(conv(rrc, cc_m))
    xb[12:28, :] = x
    bb[12:28, :] = b
    c16 = c.astype(BF16)
    carried = jnp.zeros((ROWS, 512), F32)
    for q in range(SEQ):
        one = lax.dot_general(
            c16, rootb[512 * q : 512 * q + 512, :], NT, preferred_element_type=F32
        )
        carried = jnp.where(seq == q, one, carried)
    out = jnp.exp(logs) * carried + skip * x
    for j in range(PROP):
        lo = 12 - SEQ * j
        score = jnp.sum(c * bb[lo : lo + ROWS, :], axis=-1, keepdims=True)
        out = out + score * dj[j] * xb[lo : lo + ROWS, :]
    g = out * silu(gate)
    g = g * lax.rsqrt(jnp.mean(g * g, axis=-1, keepdims=True) + EPSILON)
    nrg[at(z, ROWS), :] = (g * og_m[...]).astype(BF16)
    for d in FAR + NEAR:
        send(O1, d, nrg.at[at(z, ROWS), :], nrg.at[at(z, ROWS), :], z, over(d), tp)

    for r in range(PAST):
        nv_m[r] = rrv[SEQ * r : SEQ * r + SEQ, :].astype(BF16)
        nb_m[r] = rrb[SEQ * r : SEQ * r + SEQ, :].astype(BF16)
        nc_m[r] = rrc[SEQ * r : SEQ * r + SEQ, :].astype(BF16)

    for d in FAR + NEAR:
        yy = (y + d) % N
        arrived(OW, yy, owg.at[at(yy, 32), :])
    for d in FAR + NEAR:
        zz = (z + d) % N
        arrived(O1, zz, nrg.at[at(zz, ROWS), :])
    po[...] = lax.dot_general(nrg[...], owg[...], NT, preferred_element_type=F32).astype(BF16)

    def back(d):
        zz = (z + d) % N
        return pltpu.make_async_remote_copy(
            src_ref=po.at[at(zz, ROWS), :], dst_ref=osum.at[tp], send_sem=send_sem.at[O2, d],
            recv_sem=recv_sem.at[O2, tp], device_id=(over(d), z), device_id_type=MESH,
        )

    for d in FAR + NEAR:
        back(d).start()

    @pl.when(z != tp)
    def _():
        back(0).start()

    @pl.when(z == tp)
    def _():
        osum[tp] = po[at(z, ROWS), :]

    for d in range(1, N):
        t = (tp + d) % N
        arrived(O2, t, osum.at[t])

    @pl.when(z != tp)
    def _():
        arrived(O2, tp, osum.at[tp])

    total = osum[0].astype(F32)
    for t in range(1, N):
        total = total + osum[t].astype(F32)
    for i in range(2):
        mf[i] = total[:, 128 * i : 128 * i + 128]
        for q in range(SEQ):
            mixed_m[q, :, 128 * i : 128 * i + 128] = mf.at[i][
                pl.ds(q, PROP, stride=SEQ), :
            ].astype(BF16)

    for c in sent:
        c.wait_send()
    for d in range(1, N):
        back(d).wait_send()

    @pl.when(z != tp)
    def _():
        back(0).wait_send()


def finish(*refs):
    ins, outs, sem = refs[:6], refs[6:12], refs[12]
    copies = [pltpu.make_async_copy(s, d, sem.at[i]) for i, (s, d) in enumerate(zip(ins, outs))]
    for c in copies:
        c.start()
    for c in copies:
        c.wait()


def on_device(
    tokens, input_gain, gate_weight, value_weight, write_weight, read_weight, step_weight,
    conv_value, conv_write, conv_read, step_bias, decay_log, skip_gain, output_gain,
    out_weight, base_state, past_value, past_write, past_read, past_step, accepted,
):
    vmem = pltpu.VMEM
    ops = (
        tokens, input_gain[None, :], gate_weight, value_weight, write_weight, read_weight,
        step_weight.T, conv_value, conv_write, conv_read, step_bias[None, :],
        decay_log[None, :], skip_gain[None, :], output_gain[None, :], out_weight.T,
        base_state.reshape(2048, 128), past_value.transpose(1, 0, 2),
        past_write.transpose(1, 0, 2), past_read.transpose(1, 0, 2), past_step, accepted,
    )
    out_shapes = [
        ((SEQ, PROP, 256), BF16), ((2048, 128), F32), ((PAST, SEQ, 512), BF16),
        ((PAST, SEQ, 128), BF16), ((PAST, SEQ, 128), BF16), ((SEQ, PROP, 8), BF16),
    ]
    scratch = [
        vmem((1, 2048), F32), vmem((64, 2048), BF16), vmem((4, 512), F32), vmem((4, 128), F32),
        vmem((4, 128), F32), vmem((1, 8), F32), vmem((1, 8), F32), vmem((1, 8), F32),
        vmem((1, 512), F32), vmem((2048, 128), F32), vmem((PAST, SEQ, 512), BF16),
        vmem((PAST, SEQ, 128), BF16), vmem((PAST, SEQ, 128), BF16), vmem((SEQ, PROP, 8), BF16),
        vmem((N, SEQ, PROP, 256), BF16), vmem((N, ROWS, 256), BF16), vmem((N, ROWS, 256), BF16),
        vmem((128, 256), BF16), vmem((128, 256), BF16), vmem((256, 640), BF16),
        vmem((256, 640), BF16), vmem((128, 640), BF16), vmem((128, 640), BF16),
        vmem((N, ROWS, 640), BF16), vmem((N, ROWS, 640), BF16), vmem((256, 512), BF16),
        vmem((128, 512), BF16), vmem((128, 256), BF16), vmem((N, ROWS, 256), BF16),
        vmem((ROWS, 2048), F32), vmem((28, 512), F32), vmem((28, 128), F32), vmem((28, 128), F32),
        vmem((28, 512), F32), vmem((28, 128), F32), vmem((28, 128), F32), vmem((ROWS, 512), F32),
        vmem((ROWS, 512), F32), vmem((ROWS, 512), F32), vmem((ROWS, 128), F32),
        vmem((28, 512), F32), vmem((28, 128), F32), vmem((28, 512), F32), vmem((28, 512), F32),
        vmem((PROP, ROWS, 512), F32), vmem((2048, 128), BF16), vmem((2, ROWS, 128), F32),
        vmem((ROWS, 128), F32),
        pltpu.SMEM((SEQ,), jnp.int32),
        pltpu.SemaphoreType.DMA((21,)),
        pltpu.SemaphoreType.DMA((10, N)),
        pltpu.SemaphoreType.DMA((10, N)),
    ]
    held = pl.pallas_call(
        body,
        out_shape=[vmem(shape, dtype) for shape, dtype in out_shapes],
        in_specs=[pl.BlockSpec(memory_space=pl.ANY)] * 21,
        out_specs=[pl.BlockSpec(memory_space=vmem)] * 6,
        scratch_shapes=scratch,
        compiler_params=pltpu.CompilerParams(collective_id=0, has_side_effects=True),
        name="mixer",
    )(*ops)
    mixed, root, nv, nb, nc, ns = pl.pallas_call(
        finish,
        out_shape=[jax.ShapeDtypeStruct(shape, dtype) for shape, dtype in out_shapes],
        in_specs=[pl.BlockSpec(memory_space=vmem)] * 6,
        out_specs=[pl.BlockSpec(memory_space=pl.ANY)] * 6,
        scratch_shapes=[pltpu.SemaphoreType.DMA((6,))],
        name="finish",
    )(*(pltpu.with_memory_space_constraint(h, vmem) for h in held))
    return (
        mixed, root.reshape(base_state.shape), nv.transpose(1, 0, 2), nb.transpose(1, 0, 2),
        nc.transpose(1, 0, 2), ns,
    )


def solution(mesh):
    return jax.shard_map(
        on_device,
        mesh=mesh,
        in_specs=(
            P("kv", None, "tp"), P(), P("kv", "tp"), P("kv", "tp"), P("kv", "tp"), P("kv", "tp"),
            P(), P(None, "tp"), P(None, "tp"), P(None, "tp"), P("tp"), P("tp"), P("tp"), P("tp"),
            P("tp", "kv"), P("kv", "tp", None, None), P("kv", None, "tp"), P("kv", None, "tp"),
            P("kv", None, "tp"), P("kv", None, "tp"), P("kv"),
        ),
        out_specs=(
            P("kv", None, "tp"), P("kv", "tp", None, None), P("kv", None, "tp"),
            P("kv", None, "tp"), P("kv", None, "tp"), P("kv", None, "tp"),
        ),
        check_vma=False,
    )
```

```python
import jax
import jax.numpy as jnp
from jax import lax
from jax.experimental import pallas as pl
from jax.experimental.pallas import tpu as pltpu
from jax.sharding import PartitionSpec as P

F32 = jnp.float32
BF16 = jnp.bfloat16
MESH = pl.DeviceIdType.MESH
EPSILON = 1e-06
HIGHEST = lax.Precision.HIGHEST

N = 8
SEQ = 4
PROP = 4
ROWS = SEQ * PROP
CONV = 4
PAST = 7
NT = (((1,), (1,)), ((), ()))
TN = (((0,), (0,)), ((), ()))
ORDER = (4, 3, 5, 2, 6, 1, 7)

T1, T2Y, T2Z, WY, WZ, RSY, RSZ, OW, O1, O2 = range(10)


def silu(v):
    return v / (1.0 + jnp.exp(-v))


def softplus(v):
    return jnp.maximum(v, 0.0) + jnp.log1p(jnp.exp(-jnp.abs(v)))


def conv(buf, taps, at=0):
    total = taps[0:1, :] * buf[at : at + ROWS, :]
    for k in range(1, CONV):
        total = total + taps[k : k + 1, :] * buf[at + SEQ * k : at + SEQ * k + ROWS, :]
    return total


def body(
    tokens, input_gain, gate_w, value_w, write_w, read_w, step_w,
    conv_v, conv_b, conv_c, step_bias, decay_log, skip_gain, output_gain,
    out_w, base, past_v, past_b, past_c, past_s, accepted,
    mixed_m, root_m, nv_m, nb_m, nc_m, ns_m,
    gain_m, stepw_m, cv_m, cb_m, cc_m, bias_m, decay_m, skip_m, og_m,
    base_m, pv_m, pb_m, pc_m, ps_m,
    xall, nrm, npk, ay, az, wy, wz, py, pz, rsy, rsz, owg, nrg, po, osum,
    xf, ppv, ppb, ppc, rrv, rrb, rrc, stp, sbuf, ubuf, bbuf, xb, bb, lb, dtb, dj, rootb, mf, nsf,
    taken_m,
    in_sem, send_sem, recv_sem,
):
    kv = lax.axis_index("kv")
    tp = lax.axis_index("tp")
    z = kv // N
    y = kv % N

    def at(rows, count):
        return pl.ds(pl.multiple_of(rows * count, count), count)

    ins = [
        (value_w, wy.at[at(y, 32), pl.ds(0, 512)]),
        (write_w, wy.at[at(y, 32), pl.ds(512, 128)]),
        (gate_w, wz.at[at(z, 32), pl.ds(0, 512)]),
        (read_w, wz.at[at(z, 32), pl.ds(512, 128)]),
        (out_w, owg.at[at(y, 32), :]),
        (tokens, xall.at[tp]),
        (input_gain, gain_m),
        (past_v, pv_m),
        (past_b, pb_m),
        (past_c, pc_m),
        (past_s, ps_m),
        (conv_v, cv_m),
        (conv_b, cb_m),
        (conv_c, cc_m),
        (step_bias, bias_m),
        (decay_log, decay_m),
        (skip_gain, skip_m),
        (output_gain, og_m),
        (step_w, stepw_m),
        (base, base_m),
        (accepted, taken_m),
    ]
    loads = [pltpu.make_async_copy(s, d, in_sem.at[i]) for i, (s, d) in enumerate(ins)]
    for c in loads:
        c.start()

    barrier = pltpu.get_barrier_semaphore()

    def tell(k, t):
        pl.semaphore_signal(barrier, inc=1, device_id=(k, t), device_id_type=MESH)

    for d in range(1, N):
        tell(kv, (tp + d) % N)
        tell(z * N + (y + d) % N, tp)
        tell(((z + d) % N) * N + y, tp)

    for c in loads[:6]:
        c.wait()
    pl.semaphore_wait(barrier, 3 * (N - 1))

    sent = []

    def send(phase, d, src, dst, slot, k, t):
        c = pltpu.make_async_remote_copy(
            src_ref=src, dst_ref=dst, send_sem=send_sem.at[phase, d],
            recv_sem=recv_sem.at[phase, slot], device_id=(k, t), device_id_type=MESH,
        )
        c.start()
        sent.append(c)

    def arrived(phase, slot, ref):
        pltpu.make_async_remote_copy(
            src_ref=ref, dst_ref=ref, send_sem=send_sem.at[phase, 0],
            recv_sem=recv_sem.at[phase, slot], device_id=(kv, tp), device_id_type=MESH,
        ).wait_recv()

    def up(d):
        return z * N + (y + d) % N

    def over(d):
        return ((z + d) % N) * N + y

    def slab(owner, h):
        return pl.ds(pl.multiple_of(owner * 32 + 16 * h, 16), 16)

    def spread_own(phase, ref, me, dev):
        for d in (2, 6, 1, 7):
            send(phase, d, ref.at[at(me, 32), :], ref.at[at(me, 32), :], me, dev(d), tp)

    def spread_on(phase, ref, me, dev):
        for h, back_two, on in ((0, 6, (1, 2)), (1, 2, (7, 6))):
            owner = (me + back_two) % N
            block, part = ref.at[at(owner, 32), :], ref.at[slab(owner, h), :]
            arrived(phase, owner, block)
            send(phase, 3 + 2 * h, block, block, owner, dev(on[0]), tp)
            send(phase, 4 - 4 * h, part, part, N + h, dev(on[1]), tp)

    def spread_end(phase, ref, me):
        for d in (1, 7, 3, 5):
            owner = (me + d) % N
            arrived(phase, owner, ref.at[at(owner, 32), :])
        for h in range(2):
            arrived(phase, N + h, ref.at[slab((me + 4) % N, h), :])

    for d in range(1, N):
        send(T1, d, xall.at[tp], xall.at[tp], tp, kv, (tp + d) % N)
    spread_own(WY, wy, y, up)
    spread_own(WZ, wz, z, over)

    for c in loads[6:]:
        c.wait()
    for r in range(PAST):
        ppv[SEQ * r : SEQ * r + SEQ, :] = pv_m[r].astype(F32)
        ppb[SEQ * r : SEQ * r + SEQ, :] = pb_m[r].astype(F32)
        ppc[SEQ * r : SEQ * r + SEQ, :] = pc_m[r].astype(F32)

    for d in range(1, N):
        t = (tp + d) % N
        arrived(T1, t, xall.at[t])
    for t in range(N):
        for q in range(SEQ):
            xf[PROP * q : PROP * q + PROP, 256 * t : 256 * t + 256] = xall[t, q].astype(F32)
    rows = xf[...]
    scale = lax.rsqrt(jnp.mean(rows * rows, axis=-1, keepdims=True) + EPSILON)
    normed16 = (rows * scale * gain_m[...]).astype(BF16)
    to = lax.broadcasted_iota(jnp.int32, (ROWS, ROWS), 0)
    by = lax.broadcasted_iota(jnp.int32, (ROWS, ROWS), 1)
    swap = jnp.where((to % SEQ) * PROP + to // SEQ == by, 1.0, 0.0).astype(BF16)
    normed = jnp.dot(swap, normed16, preferred_element_type=F32)
    normed16 = normed.astype(BF16)
    for zz in range(N):
        nrm[zz] = normed16[:, 256 * zz : 256 * zz + 256]
    lane = lax.broadcasted_iota(jnp.int32, (ROWS, 128), 1) // 32
    for yy in range(N):
        for half in range(2):
            tile = None
            for i in range(4):
                start = 256 * (4 * half + i) + 128 * (yy // 4)
                shift = (32 * i - 32 * (yy % 4)) % 128
                piece = normed[:, start : start + 128]
                if shift:
                    piece = pltpu.roll(piece, shift, 1)
                tile = piece if tile is None else jnp.where(lane == i, piece, tile)
            npk[yy, :, 128 * half : 128 * half + 128] = tile.astype(BF16)
    ay[at(z, ROWS), :] = nrm[z]
    az[at(y, ROWS), :] = npk[y]
    for d in ORDER:
        zz, yy = (z + d) % N, (y + d) % N
        send(T2Y, d, nrm.at[zz], ay.at[at(z, ROWS), :], z, over(d), tp)
        send(T2Z, d, npk.at[yy], az.at[at(y, ROWS), :], y, up(d), tp)
    spread_on(WY, wy, y, up)
    spread_on(WZ, wz, z, over)

    head = lax.broadcasted_iota(jnp.int32, (1, 512), 1) // 64

    def spread(ref):
        row = jnp.zeros((1, 512), F32)
        for h in range(8):
            row = jnp.where(head == h, ref[0:1, h : h + 1], row)
        return row

    bias = spread(bias_m)
    rate = jnp.exp(spread(decay_m))
    skip = spread(skip_m)
    step16 = lax.dot_general(normed16, stepw_m[...], NT, preferred_element_type=F32).astype(BF16)
    row64 = lax.broadcasted_iota(jnp.int32, (64, 512), 0)
    own64 = (row64 - 8 * tp == lax.broadcasted_iota(jnp.int32, (64, 512), 1) // 64)
    wide = jnp.dot(step16, jnp.where(own64, 1.0, 0.0).astype(BF16), preferred_element_type=F32)
    row64 = lax.broadcasted_iota(jnp.int32, (64, 128), 0)
    pick = (row64 - 8 * tp == lax.broadcasted_iota(jnp.int32, (64, 128), 1))
    nsf[...] = jnp.dot(step16, jnp.where(pick, 1.0, 0.0).astype(BF16), preferred_element_type=F32)
    for q in range(SEQ):
        ns_m[q] = nsf[pl.ds(q, PROP, stride=SEQ), :][:, 0:8].astype(BF16)

    dt = softplus(wide + bias)
    sbuf[...] = -rate * dt
    run = jnp.zeros((SEQ, 512), F32)
    lb[0:12, :] = jnp.zeros((12, 512), F32)
    dtb[0:12, :] = jnp.zeros((12, 512), F32)
    xb[0:12, :] = jnp.zeros((12, 512), F32)
    bb[0:12, :] = jnp.zeros((12, 128), F32)
    for t in range(PROP):
        run = run + sbuf[SEQ * t : SEQ * t + SEQ, :]
        lb[12 + SEQ * t : 16 + SEQ * t, :] = run
    dtb[12:28, :] = dt
    logs = lb[12:28, :]
    for j in range(PROP):
        lo = 12 - SEQ * j
        dj[j] = jnp.exp(logs - lb[lo : lo + ROWS, :]) * dtb[lo : lo + ROWS, :]

    eight = (
        lax.broadcasted_iota(jnp.int32, (8, 512), 0)
        == lax.broadcasted_iota(jnp.int32, (8, 512), 1) // 64
    )
    eight = jnp.where(eight, 1.0, 0.0).astype(BF16)
    for q in range(SEQ):
        stp[PROP * q : PROP * q + PROP, :] = jnp.dot(
            ps_m[q], eight, preferred_element_type=F32
        )
    steps = jnp.dot(swap, stp[...].astype(BF16), preferred_element_type=F32)
    pd = softplus(steps + bias)

    def taken(shape):
        seq = lax.broadcasted_iota(jnp.int32, shape, 0) % SEQ
        count = jnp.full(shape, taken_m[0], jnp.int32)
        for q in range(1, SEQ):
            count = jnp.where(seq == q, taken_m[q], count)
        return count

    live = lax.broadcasted_iota(jnp.int32, (ROWS, 512), 0) // SEQ < taken((ROWS, 512))
    sbuf[...] = jnp.where(live, -rate * pd, 0.0)
    pls = [sbuf[SEQ * s : SEQ * s + SEQ, :] for s in range(PROP)]
    tails = [None] * PROP
    run = jnp.zeros((SEQ, 512), F32)
    for s in reversed(range(PROP)):
        tails[s] = run
        run = run + pls[s]
    kept = jnp.exp(run)
    for s in range(PROP):
        stp[SEQ * s : SEQ * s + SEQ, :] = jnp.exp(tails[s])
    ubuf[...] = jnp.where(live, stp[...] * pd, 0.0) * silu(conv(ppv, cv_m))
    bbuf[...] = silu(conv(ppb, cb_m))

    def window(pp, rr, width):
        count = taken((12, width))
        first = pp[SEQ : SEQ + 12, :]
        for a in range(2, PROP + 1):
            first = jnp.where(count == a, pp[SEQ * a : SEQ * a + 12, :], first)
        rr[0:12, :] = first

    window(ppv, rrv, 512)
    window(ppb, rrb, 128)
    window(ppc, rrc, 128)

    for d in range(1, N):
        zz, yy = (z + d) % N, (y + d) % N
        arrived(T2Y, zz, ay.at[at(zz, ROWS), :])
        arrived(T2Z, yy, az.at[at(yy, ROWS), :])
    spread_end(WY, wy, y)
    py[...] = jnp.dot(ay[...], wy[...], preferred_element_type=F32).astype(BF16)
    spread_end(WZ, wz, z)
    pz[...] = jnp.dot(az[...], wz[...], preferred_element_type=F32).astype(BF16)
    for d in ORDER:
        zz, yy = (z + d) % N, (y + d) % N
        send(RSY, d, py.at[at(zz, ROWS), :], rsy.at[z], z, over(d), tp)
        send(RSZ, d, pz.at[at(yy, ROWS), :], rsz.at[y], y, up(d), tp)
    spread_own(OW, owg, y, up)
    rsy[z] = py[at(z, ROWS), :]
    rsz[y] = pz[at(y, ROWS), :]

    seq = lax.broadcasted_iota(jnp.int32, (ROWS, 512), 0) % SEQ
    for q in range(SEQ):
        u = jnp.where(seq == q, ubuf[...], 0.0)
        grown = lax.dot_general(u, bbuf[...], TN, precision=HIGHEST, preferred_element_type=F32)
        for h in range(8):
            lo = 512 * q + 64 * h
            old = jnp.broadcast_to(kept[q : q + 1, 64 * h : 64 * h + 1], (64, 128))
            new = old * base_m[lo : lo + 64, :] + grown[64 * h : 64 * h + 64, :]
            root_m[lo : lo + 64, :] = new
            rootb[lo : lo + 64, :] = new.astype(BF16)

    for d in ORDER:
        zz, yy = (z + d) % N, (y + d) % N
        arrived(RSY, zz, rsy.at[zz])
        arrived(RSZ, yy, rsz.at[yy])

    def summed(ref, lo, hi):
        total = ref[0, :, lo:hi].astype(F32)
        for s in range(1, N):
            total = total + ref[s, :, lo:hi].astype(F32)
        return total.astype(BF16).astype(F32)

    rrv[12:28, :] = summed(rsy, 0, 512)
    rrb[12:28, :] = summed(rsy, 512, 640)
    rrc[12:28, :] = summed(rsz, 512, 640)
    gate = summed(rsz, 0, 512)
    x = silu(conv(rrv, cv_m))
    b = silu(conv(rrb, cb_m))
    c = silu(conv(rrc, cc_m))
    xb[12:28, :] = x
    bb[12:28, :] = b
    c16 = c.astype(BF16)
    carried = jnp.zeros((ROWS, 512), F32)
    for q in range(SEQ):
        one = lax.dot_general(
            c16, rootb[512 * q : 512 * q + 512, :], NT, preferred_element_type=F32
        )
        carried = jnp.where(seq == q, one, carried)
    out = jnp.exp(logs) * carried + skip * x
    for j in range(PROP):
        lo = 12 - SEQ * j
        score = jnp.sum(c * bb[lo : lo + ROWS, :], axis=-1, keepdims=True)
        out = out + score * dj[j] * xb[lo : lo + ROWS, :]
    g = out * silu(gate)
    g = g * lax.rsqrt(jnp.mean(g * g, axis=-1, keepdims=True) + EPSILON)
    nrg[at(z, ROWS), :] = (g * og_m[...]).astype(BF16)
    for d in ORDER:
        send(O1, d, nrg.at[at(z, ROWS), :], nrg.at[at(z, ROWS), :], z, over(d), tp)
    spread_on(OW, owg, y, up)

    for r in range(PAST):
        nv_m[r] = rrv[SEQ * r : SEQ * r + SEQ, :].astype(BF16)
        nb_m[r] = rrb[SEQ * r : SEQ * r + SEQ, :].astype(BF16)
        nc_m[r] = rrc[SEQ * r : SEQ * r + SEQ, :].astype(BF16)

    spread_end(OW, owg, y)
    for d in ORDER:
        zz = (z + d) % N
        arrived(O1, zz, nrg.at[at(zz, ROWS), :])
    po[...] = lax.dot_general(nrg[...], owg[...], NT, preferred_element_type=F32).astype(BF16)

    def back(d):
        zz = (z + d) % N
        return pltpu.make_async_remote_copy(
            src_ref=po.at[at(zz, ROWS), :], dst_ref=osum.at[tp], send_sem=send_sem.at[O2, d],
            recv_sem=recv_sem.at[O2, tp], device_id=(over(d), z), device_id_type=MESH,
        )

    for d in ORDER:
        back(d).start()

    @pl.when(z != tp)
    def _():
        back(0).start()

    @pl.when(z == tp)
    def _():
        osum[tp] = po[at(z, ROWS), :]

    for d in range(1, N):
        t = (tp + d) % N
        arrived(O2, t, osum.at[t])

    @pl.when(z != tp)
    def _():
        arrived(O2, tp, osum.at[tp])

    total = osum[0].astype(F32)
    for t in range(1, N):
        total = total + osum[t].astype(F32)
    for i in range(2):
        mf[i] = total[:, 128 * i : 128 * i + 128]
        for q in range(SEQ):
            mixed_m[q, :, 128 * i : 128 * i + 128] = mf.at[i][
                pl.ds(q, PROP, stride=SEQ), :
            ].astype(BF16)

    for c in sent:
        c.wait_send()
    for d in range(1, N):
        back(d).wait_send()

    @pl.when(z != tp)
    def _():
        back(0).wait_send()


def finish(*refs):
    ins, outs, sem = refs[:6], refs[6:12], refs[12]
    copies = [pltpu.make_async_copy(s, d, sem.at[i]) for i, (s, d) in enumerate(zip(ins, outs))]
    for c in copies:
        c.start()
    for c in copies:
        c.wait()


def on_device(
    tokens, input_gain, gate_weight, value_weight, write_weight, read_weight, step_weight,
    conv_value, conv_write, conv_read, step_bias, decay_log, skip_gain, output_gain,
    out_weight, base_state, past_value, past_write, past_read, past_step, accepted,
):
    vmem = pltpu.VMEM
    ops = (
        tokens, input_gain[None, :], gate_weight, value_weight, write_weight, read_weight,
        step_weight.T, conv_value, conv_write, conv_read, step_bias[None, :],
        decay_log[None, :], skip_gain[None, :], output_gain[None, :], out_weight.T,
        base_state.reshape(2048, 128), past_value.transpose(1, 0, 2),
        past_write.transpose(1, 0, 2), past_read.transpose(1, 0, 2), past_step, accepted,
    )
    out_shapes = [
        ((SEQ, PROP, 256), BF16), ((2048, 128), F32), ((PAST, SEQ, 512), BF16),
        ((PAST, SEQ, 128), BF16), ((PAST, SEQ, 128), BF16), ((SEQ, PROP, 8), BF16),
    ]
    scratch = [
        vmem((1, 2048), F32), vmem((64, 2048), BF16), vmem((4, 512), F32), vmem((4, 128), F32),
        vmem((4, 128), F32), vmem((1, 8), F32), vmem((1, 8), F32), vmem((1, 8), F32),
        vmem((1, 512), F32), vmem((2048, 128), F32), vmem((PAST, SEQ, 512), BF16),
        vmem((PAST, SEQ, 128), BF16), vmem((PAST, SEQ, 128), BF16), vmem((SEQ, PROP, 8), BF16),
        vmem((N, SEQ, PROP, 256), BF16), vmem((N, ROWS, 256), BF16), vmem((N, ROWS, 256), BF16),
        vmem((128, 256), BF16), vmem((128, 256), BF16), vmem((256, 640), BF16),
        vmem((256, 640), BF16), vmem((128, 640), BF16), vmem((128, 640), BF16),
        vmem((N, ROWS, 640), BF16), vmem((N, ROWS, 640), BF16), vmem((256, 512), BF16),
        vmem((128, 512), BF16), vmem((128, 256), BF16), vmem((N, ROWS, 256), BF16),
        vmem((ROWS, 2048), F32), vmem((28, 512), F32), vmem((28, 128), F32), vmem((28, 128), F32),
        vmem((28, 512), F32), vmem((28, 128), F32), vmem((28, 128), F32), vmem((ROWS, 512), F32),
        vmem((ROWS, 512), F32), vmem((ROWS, 512), F32), vmem((ROWS, 128), F32),
        vmem((28, 512), F32), vmem((28, 128), F32), vmem((28, 512), F32), vmem((28, 512), F32),
        vmem((PROP, ROWS, 512), F32), vmem((2048, 128), BF16), vmem((2, ROWS, 128), F32),
        vmem((ROWS, 128), F32),
        pltpu.SMEM((SEQ,), jnp.int32),
        pltpu.SemaphoreType.DMA((21,)),
        pltpu.SemaphoreType.DMA((10, N)),
        pltpu.SemaphoreType.DMA((10, N + 2)),
    ]
    held = pl.pallas_call(
        body,
        out_shape=[vmem(shape, dtype) for shape, dtype in out_shapes],
        in_specs=[pl.BlockSpec(memory_space=pl.ANY)] * 21,
        out_specs=[pl.BlockSpec(memory_space=vmem)] * 6,
        scratch_shapes=scratch,
        compiler_params=pltpu.CompilerParams(collective_id=0, has_side_effects=True),
        name="mixer",
    )(*ops)
    mixed, root, nv, nb, nc, ns = pl.pallas_call(
        finish,
        out_shape=[jax.ShapeDtypeStruct(shape, dtype) for shape, dtype in out_shapes],
        in_specs=[pl.BlockSpec(memory_space=vmem)] * 6,
        out_specs=[pl.BlockSpec(memory_space=pl.ANY)] * 6,
        scratch_shapes=[pltpu.SemaphoreType.DMA((6,))],
        name="finish",
    )(*(pltpu.with_memory_space_constraint(h, vmem) for h in held))
    return (
        mixed, root.reshape(base_state.shape), nv.transpose(1, 0, 2), nb.transpose(1, 0, 2),
        nc.transpose(1, 0, 2), ns,
    )


def solution(mesh):
    return jax.shard_map(
        on_device,
        mesh=mesh,
        in_specs=(
            P("kv", None, "tp"), P(), P("kv", "tp"), P("kv", "tp"), P("kv", "tp"), P("kv", "tp"),
            P(), P(None, "tp"), P(None, "tp"), P(None, "tp"), P("tp"), P("tp"), P("tp"), P("tp"),
            P("tp", "kv"), P("kv", "tp", None, None), P("kv", None, "tp"), P("kv", None, "tp"),
            P("kv", None, "tp"), P("kv", None, "tp"), P("kv"),
        ),
        out_specs=(
            P("kv", None, "tp"), P("kv", "tp", None, None), P("kv", None, "tp"),
            P("kv", None, "tp"), P("kv", None, "tp"), P("kv", None, "tp"),
        ),
        check_vma=False,
    )
```

```python
import jax
import jax.numpy as jnp
from jax import lax
from jax.experimental import pallas as pl
from jax.experimental.pallas import tpu as pltpu
from jax.sharding import PartitionSpec as P

F32 = jnp.float32
BF16 = jnp.bfloat16
MESH = pl.DeviceIdType.MESH
EPSILON = 1e-06
HIGHEST = lax.Precision.HIGHEST

N = 8
SEQ = 4
PROP = 4
ROWS = SEQ * PROP
CONV = 4
PAST = 7
NT = (((1,), (1,)), ((), ()))
TN = (((0,), (0,)), ((), ()))
ORDER = (4, 3, 5, 2, 6, 1, 7)

T1, T2Y, T2Z, WY, WZ, RSY, RSZ, OW, O1, O2 = range(10)


def silu(v):
    return v / (1.0 + jnp.exp(-v))


def softplus(v):
    return jnp.maximum(v, 0.0) + jnp.log1p(jnp.exp(-jnp.abs(v)))


def conv(buf, taps, at=0):
    total = taps[0:1, :] * buf[at : at + ROWS, :]
    for k in range(1, CONV):
        total = total + taps[k : k + 1, :] * buf[at + SEQ * k : at + SEQ * k + ROWS, :]
    return total


def body(
    tokens, input_gain, gate_w, value_w, write_w, read_w, step_w,
    conv_v, conv_b, conv_c, step_bias, decay_log, skip_gain, output_gain,
    out_w, base, past_v, past_b, past_c, past_s, accepted,
    mixed_m, root_m, nv_m, nb_m, nc_m, ns_m,
    gain_m, stepw_m, cv_m, cb_m, cc_m, bias_m, decay_m, skip_m, og_m,
    base_m, pv_m, pb_m, pc_m, ps_m, tok_m,
    xall, nrm, npk, ay, az, wy, wz, py, pz, rsy, rsz, owg, nrg, po, osum,
    xf, ppv, ppb, ppc, rrv, rrb, rrc, stp, sbuf, ubuf, bbuf, xb, bb, lb, dtb, dj, rootb, mf, nsf,
    taken_m,
    in_sem, send_sem, recv_sem, hello,
):
    kv = lax.axis_index("kv")
    tp = lax.axis_index("tp")
    z = kv // N
    y = kv % N

    def at(rows, count):
        return pl.ds(pl.multiple_of(rows * count, count), count)

    def up(d):
        return z * N + (y + d) % N

    def over(d):
        return ((z + d) % N) * N + y

    groups = (
        (
            (value_w, wy.at[at(y, 32), pl.ds(0, 512)]),
            (write_w, wy.at[at(y, 32), pl.ds(512, 128)]),
            (gate_w, wz.at[at(z, 32), pl.ds(0, 512)]),
            (read_w, wz.at[at(z, 32), pl.ds(512, 128)]),
            (out_w, owg.at[at(y, 32), :]),
            (tokens, tok_m),
        ),
        (
            (input_gain, gain_m),
            (past_v, pv_m),
            (past_b, pb_m),
            (past_c, pc_m),
            (conv_v, cv_m),
            (conv_b, cb_m),
            (conv_c, cc_m),
            (output_gain, og_m),
        ),
        ((past_s, ps_m),),
        ((step_bias, bias_m),),
        ((decay_log, decay_m),),
        ((skip_gain, skip_m),),
        ((accepted, taken_m),),
        ((step_w, stepw_m),),
        ((base, base_m),),
    )
    for i, group in enumerate(groups):
        for source, target in group:
            pltpu.make_async_copy(source, target, in_sem.at[i]).start()

    def loaded(i, ref=None):
        if ref is None:
            pltpu.make_async_copy(*groups[i][0], in_sem.at[i]).wait()
        else:
            pltpu.make_async_copy(ref, ref, in_sem.at[i]).wait()

    barrier = pltpu.get_barrier_semaphore()

    def tell(k, t):
        pl.semaphore_signal(barrier, inc=1, device_id=(k, t), device_id_type=MESH)

    for d in range(1, N):
        tell(kv, (tp + d) % N)
    for d in (1, 7, 2, 6):
        tell(up(d), tp)
        tell(over(d), tp)

    loaded(0, wy.at[pl.ds(0, 96), :])
    to = lax.broadcasted_iota(jnp.int32, (ROWS, ROWS), 0)
    by = lax.broadcasted_iota(jnp.int32, (ROWS, ROWS), 1)
    swap = jnp.where((to % SEQ) * PROP + to // SEQ == by, 1.0, 0.0).astype(BF16)
    for q in range(SEQ):
        xf[PROP * q : PROP * q + PROP, :] = tok_m[q].astype(F32)
    xall[tp] = jnp.dot(swap, xf[...].astype(BF16), preferred_element_type=F32).astype(BF16)
    pl.semaphore_wait(barrier, N - 1 + 8)
    for d in (2, 6):
        pl.semaphore_signal(hello, inc=1, device_id=(up(d), tp), device_id_type=MESH)
        pl.semaphore_signal(hello, inc=1, device_id=(over(d), tp), device_id_type=MESH)

    def copy(phase, slot, src, dst, k, t):
        return pltpu.make_async_remote_copy(
            src_ref=src, dst_ref=dst, send_sem=send_sem.at[phase], recv_sem=recv_sem.at[slot],
            device_id=(k, t), device_id_type=MESH,
        )

    def send(phase, src, dst, k, t):
        copy(phase, phase, src, dst, k, t).start()

    def arrived(phase, ref):
        copy(phase, phase, ref, ref, kv, tp).wait_recv()

    def gone(phase, ref):
        copy(phase, phase, ref, ref, kv, tp).wait_send()

    def slab(ref, owner, h):
        return ref.at[pl.ds(pl.multiple_of(owner * 32 + 16 * h, 16), 16), :]

    def pass_slab(phase, slot, ref, owner, h, k):
        copy(phase, slot, slab(ref, owner, h), slab(ref, owner, h), k, tp).start()

    def early(first, h, side):
        return first + 2 * h + side

    def spread_own(rings):
        for ds in ((2, 6), (1, 7)):
            for h in range(2):
                for side, d in enumerate(ds):
                    for phase, first, ref, me, dev in rings:
                        slot = early(first, h, side) if d in (2, 6) else phase
                        pass_slab(phase, slot, ref, me, h, dev(d))

    def spread_on(rings):
        for h in range(2):
            for side, (back_two, one, two) in enumerate(((6, 1, 2), (2, 7, 6))):
                for phase, first, ref, me, dev in rings:
                    owner = (me + back_two) % N
                    part = slab(ref, owner, h)
                    copy(phase, early(first, h, side), part, part, kv, tp).wait_recv()
                    pass_slab(phase, phase, ref, owner, h, dev(one))
                    if h == side:
                        pass_slab(phase, phase, ref, owner, h, dev(two))

    def spread_end(ring):
        arrived(ring[0], ring[2].at[pl.ds(0, 160), :])

    ring_y = (WY, 10, wy, y, up)
    ring_z = (WZ, 14, wz, z, over)
    ring_o = (OW, 18, owg, y, up)

    for d in range(1, N):
        send(T1, xall.at[tp], xall.at[tp], kv, (tp + d) % N)
    spread_own((ring_y, ring_z))

    loaded(1, base_m.at[pl.ds(0, 128), :])
    for i in range(2, 9):
        loaded(i)
    for r in range(PAST):
        ppv[SEQ * r : SEQ * r + SEQ, :] = pv_m[r].astype(F32)
        ppb[SEQ * r : SEQ * r + SEQ, :] = pb_m[r].astype(F32)
        ppc[SEQ * r : SEQ * r + SEQ, :] = pc_m[r].astype(F32)

    arrived(T1, xall.at[pl.ds(0, N - 1)])
    blocks = [xall[t].astype(F32) for t in range(N)]
    square = blocks[0] * blocks[0]
    for t in range(1, N):
        square = square + blocks[t] * blocks[t]
    scale = lax.rsqrt(jnp.sum(square, axis=-1, keepdims=True) * (1.0 / 2048) + EPSILON)
    normed = []
    for t in range(N):
        block = (blocks[t] * scale * gain_m[:, 256 * t : 256 * t + 256]).astype(BF16)
        nrm[t] = block
        normed.append(block.astype(F32))
    ay[at(z, ROWS), :] = nrm[z]
    pl.semaphore_wait(hello, 4)
    for d in ORDER:
        zz = (z + d) % N
        send(T2Y, nrm.at[zz], ay.at[at(z, ROWS), :], over(d), tp)
    lane = lax.broadcasted_iota(jnp.int32, (ROWS, 128), 1) // 32
    for yy in range(N):
        for half in range(2):
            tile = None
            for i in range(4):
                shift = (32 * i - 32 * (yy % 4)) % 128
                start = 128 * (yy // 4)
                piece = normed[4 * half + i][:, start : start + 128]
                if shift:
                    piece = pltpu.roll(piece, shift, 1)
                tile = piece if tile is None else jnp.where(lane == i, piece, tile)
            npk[yy, :, 128 * half : 128 * half + 128] = tile.astype(BF16)
    az[at(y, ROWS), :] = npk[y]
    for d in ORDER:
        yy = (y + d) % N
        send(T2Z, npk.at[yy], az.at[at(y, ROWS), :], up(d), tp)
    spread_on((ring_y, ring_z))

    head = lax.broadcasted_iota(jnp.int32, (1, 512), 1) // 64

    def spread(ref):
        row = jnp.zeros((1, 512), F32)
        for h in range(8):
            row = jnp.where(head == h, ref[0:1, h : h + 1], row)
        return row

    bias = spread(bias_m)
    rate = jnp.exp(spread(decay_m))
    skip = spread(skip_m)
    step = jnp.zeros((ROWS, 64), F32)
    for t in range(N):
        weight = stepw_m[:, 256 * t : 256 * t + 256]
        step = step + lax.dot_general(nrm[t], weight, NT, preferred_element_type=F32)
    step16 = step.astype(BF16)
    row64 = lax.broadcasted_iota(jnp.int32, (64, 512), 0)
    own64 = (row64 - 8 * tp == lax.broadcasted_iota(jnp.int32, (64, 512), 1) // 64)
    wide = jnp.dot(step16, jnp.where(own64, 1.0, 0.0).astype(BF16), preferred_element_type=F32)
    row64 = lax.broadcasted_iota(jnp.int32, (64, 128), 0)
    pick = (row64 - 8 * tp == lax.broadcasted_iota(jnp.int32, (64, 128), 1))
    nsf[...] = jnp.dot(step16, jnp.where(pick, 1.0, 0.0).astype(BF16), preferred_element_type=F32)
    for q in range(SEQ):
        ns_m[q] = nsf[pl.ds(q, PROP, stride=SEQ), :][:, 0:8].astype(BF16)

    dt = softplus(wide + bias)
    sbuf[...] = -rate * dt
    run = jnp.zeros((SEQ, 512), F32)
    lb[0:12, :] = jnp.zeros((12, 512), F32)
    dtb[0:12, :] = jnp.zeros((12, 512), F32)
    xb[0:12, :] = jnp.zeros((12, 512), F32)
    bb[0:12, :] = jnp.zeros((12, 128), F32)
    for t in range(PROP):
        run = run + sbuf[SEQ * t : SEQ * t + SEQ, :]
        lb[12 + SEQ * t : 16 + SEQ * t, :] = run
    dtb[12:28, :] = dt
    logs = lb[12:28, :]
    for j in range(PROP):
        lo = 12 - SEQ * j
        dj[j] = jnp.exp(logs - lb[lo : lo + ROWS, :]) * dtb[lo : lo + ROWS, :]

    eight = (
        lax.broadcasted_iota(jnp.int32, (8, 512), 0)
        == lax.broadcasted_iota(jnp.int32, (8, 512), 1) // 64
    )
    eight = jnp.where(eight, 1.0, 0.0).astype(BF16)
    for q in range(SEQ):
        stp[PROP * q : PROP * q + PROP, :] = jnp.dot(
            ps_m[q], eight, preferred_element_type=F32
        )
    steps = jnp.dot(swap, stp[...].astype(BF16), preferred_element_type=F32)
    pd = softplus(steps + bias)

    def taken(shape):
        seq = lax.broadcasted_iota(jnp.int32, shape, 0) % SEQ
        count = jnp.full(shape, taken_m[0], jnp.int32)
        for q in range(1, SEQ):
            count = jnp.where(seq == q, taken_m[q], count)
        return count

    live = lax.broadcasted_iota(jnp.int32, (ROWS, 512), 0) // SEQ < taken((ROWS, 512))
    sbuf[...] = jnp.where(live, -rate * pd, 0.0)
    pls = [sbuf[SEQ * s : SEQ * s + SEQ, :] for s in range(PROP)]
    tails = [None] * PROP
    run = jnp.zeros((SEQ, 512), F32)
    for s in reversed(range(PROP)):
        tails[s] = run
        run = run + pls[s]
    kept = jnp.exp(run)
    for s in range(PROP):
        stp[SEQ * s : SEQ * s + SEQ, :] = jnp.exp(tails[s])
    ubuf[...] = jnp.where(live, stp[...] * pd, 0.0) * silu(conv(ppv, cv_m))
    bbuf[...] = silu(conv(ppb, cb_m))

    def window(pp, rr, width):
        count = taken((12, width))
        first = pp[SEQ : SEQ + 12, :]
        for a in range(2, PROP + 1):
            first = jnp.where(count == a, pp[SEQ * a : SEQ * a + 12, :], first)
        rr[0:12, :] = first

    window(ppv, rrv, 512)
    window(ppb, rrb, 128)
    window(ppc, rrc, 128)

    rest = pl.ds(0, ROWS * (N - 1))
    arrived(T2Y, ay.at[rest, :])
    arrived(T2Z, az.at[rest, :])
    spread_end(ring_y)
    py[...] = jnp.dot(ay[...], wy[...], preferred_element_type=F32).astype(BF16)
    spread_end(ring_z)
    pz[...] = jnp.dot(az[...], wz[...], preferred_element_type=F32).astype(BF16)
    for d in ORDER:
        zz, yy = (z + d) % N, (y + d) % N
        send(RSY, py.at[at(zz, ROWS), :], rsy.at[z], over(d), tp)
        send(RSZ, pz.at[at(yy, ROWS), :], rsz.at[y], up(d), tp)
    rsy[z] = py[at(z, ROWS), :]
    rsz[y] = pz[at(y, ROWS), :]

    seq = lax.broadcasted_iota(jnp.int32, (ROWS, 512), 0) % SEQ
    for q in range(SEQ):
        u = jnp.where(seq == q, ubuf[...], 0.0)
        grown = lax.dot_general(u, bbuf[...], TN, precision=HIGHEST, preferred_element_type=F32)
        for h in range(8):
            lo = 512 * q + 64 * h
            old = jnp.broadcast_to(kept[q : q + 1, 64 * h : 64 * h + 1], (64, 128))
            new = old * base_m[lo : lo + 64, :] + grown[64 * h : 64 * h + 64, :]
            root_m[lo : lo + 64, :] = new
            rootb[lo : lo + 64, :] = new.astype(BF16)

    spread_own((ring_o,))

    arrived(RSY, rsy.at[pl.ds(0, N - 1)])
    arrived(RSZ, rsz.at[pl.ds(0, N - 1)])

    def summed(ref, lo, hi):
        total = ref[0, :, lo:hi].astype(F32)
        for s in range(1, N):
            total = total + ref[s, :, lo:hi].astype(F32)
        return total.astype(BF16).astype(F32)

    rrv[12:28, :] = summed(rsy, 0, 512)
    rrb[12:28, :] = summed(rsy, 512, 640)
    rrc[12:28, :] = summed(rsz, 512, 640)
    gate = summed(rsz, 0, 512)
    x = silu(conv(rrv, cv_m))
    b = silu(conv(rrb, cb_m))
    c = silu(conv(rrc, cc_m))
    xb[12:28, :] = x
    bb[12:28, :] = b
    c16 = c.astype(BF16)
    carried = jnp.zeros((ROWS, 512), F32)
    for q in range(SEQ):
        one = lax.dot_general(
            c16, rootb[512 * q : 512 * q + 512, :], NT, preferred_element_type=F32
        )
        carried = jnp.where(seq == q, one, carried)
    out = jnp.exp(logs) * carried + skip * x
    for j in range(PROP):
        lo = 12 - SEQ * j
        score = jnp.sum(c * bb[lo : lo + ROWS, :], axis=-1, keepdims=True)
        out = out + score * dj[j] * xb[lo : lo + ROWS, :]
    g = out * silu(gate)
    g = g * lax.rsqrt(jnp.mean(g * g, axis=-1, keepdims=True) + EPSILON)
    nrg[at(z, ROWS), :] = (g * og_m[...]).astype(BF16)
    for d in ORDER:
        send(O1, nrg.at[at(z, ROWS), :], nrg.at[at(z, ROWS), :], over(d), tp)
    spread_on((ring_o,))

    for r in range(PAST):
        nv_m[r] = rrv[SEQ * r : SEQ * r + SEQ, :].astype(BF16)
        nb_m[r] = rrb[SEQ * r : SEQ * r + SEQ, :].astype(BF16)
        nc_m[r] = rrc[SEQ * r : SEQ * r + SEQ, :].astype(BF16)

    spread_end(ring_o)
    arrived(O1, nrg.at[rest, :])
    po[...] = lax.dot_general(nrg[...], owg[...], NT, preferred_element_type=F32).astype(BF16)

    def back(d):
        zz = (z + d) % N
        send(O2, po.at[at(zz, ROWS), :], osum.at[tp], over(d), z)

    for d in ORDER:
        back(d)

    @pl.when(z != tp)
    def _():
        back(0)
        arrived(O2, osum)

    @pl.when(z == tp)
    def _():
        osum[tp] = po[at(z, ROWS), :]
        arrived(O2, osum.at[pl.ds(0, N - 1)])

    total = osum[0].astype(F32)
    for t in range(1, N):
        total = total + osum[t].astype(F32)
    for i in range(2):
        mf[i] = total[:, 128 * i : 128 * i + 128]
        for q in range(SEQ):
            mixed_m[q, :, 128 * i : 128 * i + 128] = mf.at[i][
                pl.ds(q, PROP, stride=SEQ), :
            ].astype(BF16)

    gone(T1, xall.at[pl.ds(0, N - 1)])
    gone(T2Y, ay.at[rest, :])
    gone(T2Z, az.at[rest, :])
    gone(WY, wy.at[pl.ds(0, 224), :])
    gone(WZ, wz.at[pl.ds(0, 224), :])
    gone(RSY, rsy.at[pl.ds(0, N - 1)])
    gone(RSZ, rsz.at[pl.ds(0, N - 1)])
    gone(OW, owg.at[pl.ds(0, 224), :])
    gone(O1, nrg.at[rest, :])

    @pl.when(z != tp)
    def _():
        gone(O2, osum)

    @pl.when(z == tp)
    def _():
        gone(O2, osum.at[pl.ds(0, N - 1)])


def finish(*refs):
    ins, outs, sem = refs[:6], refs[6:12], refs[12]
    pairs = [(s, d) for i, (s, d) in enumerate(zip(ins, outs)) if i != 1]
    pairs += [(ins[1].at[part], outs[1].at[part]) for part in (pl.ds(512 * i, 512) for i in range(4))]
    copies = [pltpu.make_async_copy(s, d, sem.at[i]) for i, (s, d) in enumerate(pairs)]
    for c in copies:
        c.start()
    for c in copies:
        c.wait()


def on_device(
    tokens, input_gain, gate_weight, value_weight, write_weight, read_weight, step_weight,
    conv_value, conv_write, conv_read, step_bias, decay_log, skip_gain, output_gain,
    out_weight, base_state, past_value, past_write, past_read, past_step, accepted,
):
    vmem = pltpu.VMEM
    ops = (
        tokens, input_gain[None, :], gate_weight, value_weight, write_weight, read_weight,
        step_weight.T, conv_value, conv_write, conv_read, step_bias[None, :],
        decay_log[None, :], skip_gain[None, :], output_gain[None, :], out_weight.T,
        base_state.reshape(2048, 128), past_value.transpose(1, 0, 2),
        past_write.transpose(1, 0, 2), past_read.transpose(1, 0, 2), past_step, accepted,
    )
    out_shapes = [
        ((SEQ, PROP, 256), BF16), ((2048, 128), F32), ((PAST, SEQ, 512), BF16),
        ((PAST, SEQ, 128), BF16), ((PAST, SEQ, 128), BF16), ((SEQ, PROP, 8), BF16),
    ]
    scratch = [
        vmem((1, 2048), F32), vmem((64, 2048), BF16), vmem((4, 512), F32), vmem((4, 128), F32),
        vmem((4, 128), F32), vmem((1, 8), F32), vmem((1, 8), F32), vmem((1, 8), F32),
        vmem((1, 512), F32), vmem((2048, 128), F32), vmem((PAST, SEQ, 512), BF16),
        vmem((PAST, SEQ, 128), BF16), vmem((PAST, SEQ, 128), BF16), vmem((SEQ, PROP, 8), BF16),
        vmem((SEQ, PROP, 256), BF16),
        vmem((N, ROWS, 256), BF16), vmem((N, ROWS, 256), BF16), vmem((N, ROWS, 256), BF16),
        vmem((128, 256), BF16), vmem((128, 256), BF16), vmem((256, 640), BF16),
        vmem((256, 640), BF16), vmem((128, 640), BF16), vmem((128, 640), BF16),
        vmem((N, ROWS, 640), BF16), vmem((N, ROWS, 640), BF16), vmem((256, 512), BF16),
        vmem((128, 512), BF16), vmem((128, 256), BF16), vmem((N, ROWS, 256), BF16),
        vmem((ROWS, 256), F32), vmem((28, 512), F32), vmem((28, 128), F32), vmem((28, 128), F32),
        vmem((28, 512), F32), vmem((28, 128), F32), vmem((28, 128), F32), vmem((ROWS, 512), F32),
        vmem((ROWS, 512), F32), vmem((ROWS, 512), F32), vmem((ROWS, 128), F32),
        vmem((28, 512), F32), vmem((28, 128), F32), vmem((28, 512), F32), vmem((28, 512), F32),
        vmem((PROP, ROWS, 512), F32), vmem((2048, 128), BF16), vmem((2, ROWS, 128), F32),
        vmem((ROWS, 128), F32),
        pltpu.SMEM((SEQ,), jnp.int32),
        pltpu.SemaphoreType.DMA((9,)),
        pltpu.SemaphoreType.DMA((10,)),
        pltpu.SemaphoreType.DMA((22,)),
        pltpu.SemaphoreType.REGULAR,
    ]
    held = pl.pallas_call(
        body,
        out_shape=[vmem(shape, dtype) for shape, dtype in out_shapes],
        in_specs=[pl.BlockSpec(memory_space=pl.ANY)] * 21,
        out_specs=[pl.BlockSpec(memory_space=vmem)] * 6,
        scratch_shapes=scratch,
        compiler_params=pltpu.CompilerParams(collective_id=0, has_side_effects=True),
        name="mixer",
    )(*ops)
    mixed, root, nv, nb, nc, ns = pl.pallas_call(
        finish,
        out_shape=[jax.ShapeDtypeStruct(shape, dtype) for shape, dtype in out_shapes],
        in_specs=[pl.BlockSpec(memory_space=vmem)] * 6,
        out_specs=[pl.BlockSpec(memory_space=pl.ANY)] * 6,
        scratch_shapes=[pltpu.SemaphoreType.DMA((9,))],
        name="finish",
    )(*(pltpu.with_memory_space_constraint(h, vmem) for h in held))
    return (
        mixed, root.reshape(base_state.shape), nv.transpose(1, 0, 2), nb.transpose(1, 0, 2),
        nc.transpose(1, 0, 2), ns,
    )


def solution(mesh):
    return jax.shard_map(
        on_device,
        mesh=mesh,
        in_specs=(
            P("kv", None, "tp"), P(), P("kv", "tp"), P("kv", "tp"), P("kv", "tp"), P("kv", "tp"),
            P(), P(None, "tp"), P(None, "tp"), P(None, "tp"), P("tp"), P("tp"), P("tp"), P("tp"),
            P("tp", "kv"), P("kv", "tp", None, None), P("kv", None, "tp"), P("kv", None, "tp"),
            P("kv", None, "tp"), P("kv", None, "tp"), P("kv"),
        ),
        out_specs=(
            P("kv", None, "tp"), P("kv", "tp", None, None), P("kv", None, "tp"),
            P("kv", None, "tp"), P("kv", None, "tp"), P("kv", None, "tp"),
        ),
        check_vma=False,
    )
```

```python
import jax
import jax.numpy as jnp
from jax import lax
from jax.experimental import pallas as pl
from jax.experimental.pallas import tpu as pltpu
from jax.sharding import PartitionSpec as P

F32 = jnp.float32
BF16 = jnp.bfloat16
MESH = pl.DeviceIdType.MESH
EPSILON = 1e-06
HIGHEST = lax.Precision.HIGHEST

N = 8
SEQ = 4
PROP = 4
ROWS = SEQ * PROP
CONV = 4
PAST = 7
NT = (((1,), (1,)), ((), ()))
TN = (((0,), (0,)), ((), ()))
ORDER = (4, 3, 5, 2, 6, 1, 7)

T1, T2Y, T2Z, WY, WZ, RSY, RSZ, OW, O1, O2 = range(10)
LATE = 22


def silu(v):
    return v / (1.0 + jnp.exp(-v))


def softplus(v):
    return jnp.maximum(v, 0.0) + jnp.log1p(jnp.exp(-jnp.abs(v)))


def conv(buf, taps, at=0):
    total = taps[0:1, :] * buf[at : at + ROWS, :]
    for k in range(1, CONV):
        total = total + taps[k : k + 1, :] * buf[at + SEQ * k : at + SEQ * k + ROWS, :]
    return total


def body(
    tokens, input_gain, gate_w, value_w, write_w, read_w, step_w,
    conv_v, conv_b, conv_c, step_bias, decay_log, skip_gain, output_gain,
    out_w, base, past_v, past_b, past_c, past_s, accepted,
    mixed_m, root_m, nv_m, nb_m, nc_m, ns_m,
    gain_m, stepw_m, cv_m, cb_m, cc_m, bias_m, decay_m, skip_m, og_m,
    base_m, pv_m, pb_m, pc_m, ps_m, tok_m,
    xall, nrm, npk, ay, az, wy, wz, py, pz, rsy, rsz, owg, nrg, po, osum,
    xf, ppv, ppb, ppc, rrv, rrb, rrc, stp, sbuf, ubuf, bbuf, xb, bb, lb, dtb, dj, rootb, mf, nsf,
    taken_m,
    in_sem, send_sem, recv_sem, hello,
):
    kv = lax.axis_index("kv")
    tp = lax.axis_index("tp")
    z = lax.div(kv, N)
    y = lax.rem(kv, N)

    def at(rows, count):
        return pl.ds(pl.multiple_of(rows * count, count), count)

    def up(d):
        return z * N + lax.rem(y + d, N)

    def over(d):
        return (lax.rem(z + d, N)) * N + y

    groups = (
        (
            (value_w, wy.at[at(y, 32), pl.ds(0, 512)]),
            (write_w, wy.at[at(y, 32), pl.ds(512, 128)]),
            (gate_w, wz.at[at(z, 32), pl.ds(0, 512)]),
            (read_w, wz.at[at(z, 32), pl.ds(512, 128)]),
            (out_w, owg.at[at(y, 32), :]),
            (tokens, tok_m),
        ),
        (
            (input_gain, gain_m),
            (past_v, pv_m),
            (past_b, pb_m),
            (past_c, pc_m),
            (conv_v, cv_m),
            (conv_b, cb_m),
            (conv_c, cc_m),
            (output_gain, og_m),
        ),
        ((past_s, ps_m),),
        ((step_bias, bias_m),),
        ((decay_log, decay_m),),
        ((skip_gain, skip_m),),
        ((accepted, taken_m),),
        ((step_w, stepw_m),),
        ((base, base_m),),
    )
    for i, group in enumerate(groups):
        for source, target in group:
            pltpu.make_async_copy(source, target, in_sem.at[i]).start()

    def loaded(i, ref=None):
        if ref is None:
            pltpu.make_async_copy(*groups[i][0], in_sem.at[i]).wait()
        else:
            pltpu.make_async_copy(ref, ref, in_sem.at[i]).wait()

    barrier = pltpu.get_barrier_semaphore()

    def tell(k, t):
        pl.semaphore_signal(barrier, inc=1, device_id=(k, t), device_id_type=MESH)

    for d in range(1, N):
        tell(kv, lax.rem(tp + d, N))
    for d in (1, 7, 2, 6):
        tell(up(d), tp)
        tell(over(d), tp)

    loaded(0, wy.at[pl.ds(0, 96), :])
    to = lax.broadcasted_iota(jnp.int32, (ROWS, ROWS), 0)
    by = lax.broadcasted_iota(jnp.int32, (ROWS, ROWS), 1)
    swap = jnp.where((to % SEQ) * PROP + to // SEQ == by, 1.0, 0.0).astype(BF16)
    for q in range(SEQ):
        xf[PROP * q : PROP * q + PROP, :] = tok_m[q].astype(F32)
    xall[tp] = jnp.dot(swap, xf[...].astype(BF16), preferred_element_type=F32).astype(BF16)
    pl.semaphore_wait(barrier, N - 1 + 8)
    for d in (2, 6):
        pl.semaphore_signal(hello, inc=1, device_id=(up(d), tp), device_id_type=MESH)
        pl.semaphore_signal(hello, inc=1, device_id=(over(d), tp), device_id_type=MESH)

    def copy(phase, slot, src, dst, k, t):
        return pltpu.make_async_remote_copy(
            src_ref=src, dst_ref=dst, send_sem=send_sem.at[phase], recv_sem=recv_sem.at[slot],
            device_id=(k, t), device_id_type=MESH,
        )

    def send(phase, src, dst, k, t):
        copy(phase, phase, src, dst, k, t).start()

    def arrived(phase, ref):
        copy(phase, phase, ref, ref, kv, tp).wait_recv()

    def gone(phase, ref):
        copy(phase, phase, ref, ref, kv, tp).wait_send()

    def slab(ref, owner, h):
        return ref.at[pl.ds(pl.multiple_of(owner * 32 + 16 * h, 16), 16), :]

    def pass_slab(phase, slot, ref, owner, h, k):
        copy(phase, slot, slab(ref, owner, h), slab(ref, owner, h), k, tp).start()

    def early(first, h, side):
        return first + 2 * h + side

    def spread_own(rings):
        for ds in ((2, 6), (1, 7)):
            for h in range(2):
                for side, d in enumerate(ds):
                    for phase, first, ref, me, dev in rings:
                        slot = early(first, h, side) if d in (2, 6) else phase
                        pass_slab(phase, slot, ref, me, h, dev(d))

    def spread_far(rings):
        for h in range(2):
            for phase, first, ref, me, dev in rings:
                pass_slab(phase, phase, ref, me, h, dev(4))

    def spread_on(rings):
        for h in range(2):
            for side, (back_two, one) in enumerate(((6, 1), (2, 7))):
                for phase, first, ref, me, dev in rings:
                    owner = lax.rem(me + back_two, N)
                    part = slab(ref, owner, h)
                    copy(phase, early(first, h, side), part, part, kv, tp).wait_recv()
                    pass_slab(phase, phase, ref, owner, h, dev(one))

    def spread_end(ring):
        arrived(ring[0], ring[2].at[pl.ds(0, 160), :])

    ring_y = (WY, 10, wy, y, up)
    ring_z = (WZ, 14, wz, z, over)
    ring_o = (OW, 18, owg, y, up)

    for d in range(1, N):
        send(T1, xall.at[tp], xall.at[tp], kv, lax.rem(tp + d, N))
    spread_own((ring_y, ring_z))

    loaded(1, base_m.at[pl.ds(0, 128), :])
    for i in range(2, 9):
        loaded(i)
    for r in range(PAST):
        ppv[SEQ * r : SEQ * r + SEQ, :] = pv_m[r].astype(F32)
        ppb[SEQ * r : SEQ * r + SEQ, :] = pb_m[r].astype(F32)
        ppc[SEQ * r : SEQ * r + SEQ, :] = pc_m[r].astype(F32)

    pl.semaphore_wait(hello, 4)
    spread_far((ring_y, ring_z))

    arrived(T1, xall.at[pl.ds(0, N - 1)])
    blocks = [xall[t].astype(F32) for t in range(N)]
    square = blocks[0] * blocks[0]
    for t in range(1, N):
        square = square + blocks[t] * blocks[t]
    scale = lax.rsqrt(jnp.sum(square, axis=-1, keepdims=True) * (1.0 / 2048) + EPSILON)
    normed = []
    for t in range(N):
        block = (blocks[t] * scale * gain_m[:, 256 * t : 256 * t + 256]).astype(BF16)
        nrm[t] = block
        normed.append(block.astype(F32))
    ay[at(z, ROWS), :] = nrm[z]
    for d in ORDER:
        zz = lax.rem(z + d, N)
        send(T2Y, nrm.at[zz], ay.at[at(z, ROWS), :], over(d), tp)
    lane = lax.broadcasted_iota(jnp.int32, (ROWS, 128), 1) // 32
    for yy in range(N):
        for half in range(2):
            tile = None
            for i in range(4):
                shift = (32 * i - 32 * (yy % 4)) % 128
                start = 128 * (yy // 4)
                piece = normed[4 * half + i][:, start : start + 128]
                if shift:
                    piece = pltpu.roll(piece, shift, 1)
                tile = piece if tile is None else jnp.where(lane == i, piece, tile)
            npk[yy, :, 128 * half : 128 * half + 128] = tile.astype(BF16)
    az[at(y, ROWS), :] = npk[y]
    for d in ORDER:
        yy = lax.rem(y + d, N)
        send(T2Z, npk.at[yy], az.at[at(y, ROWS), :], up(d), tp)
    spread_on((ring_y, ring_z))

    head = lax.broadcasted_iota(jnp.int32, (1, 512), 1) // 64

    def spread(ref):
        row = jnp.zeros((1, 512), F32)
        for h in range(8):
            row = jnp.where(head == h, ref[0:1, h : h + 1], row)
        return row

    bias = spread(bias_m)
    rate = jnp.exp(spread(decay_m))
    skip = spread(skip_m)
    step = jnp.zeros((ROWS, 64), F32)
    for t in range(N):
        weight = stepw_m[:, 256 * t : 256 * t + 256]
        step = step + lax.dot_general(nrm[t], weight, NT, preferred_element_type=F32)
    step16 = step.astype(BF16)
    row64 = lax.broadcasted_iota(jnp.int32, (64, 512), 0)
    own64 = (row64 - 8 * tp == lax.broadcasted_iota(jnp.int32, (64, 512), 1) // 64)
    wide = jnp.dot(step16, jnp.where(own64, 1.0, 0.0).astype(BF16), preferred_element_type=F32)
    row64 = lax.broadcasted_iota(jnp.int32, (64, 128), 0)
    pick = (row64 - 8 * tp == lax.broadcasted_iota(jnp.int32, (64, 128), 1))
    nsf[...] = jnp.dot(step16, jnp.where(pick, 1.0, 0.0).astype(BF16), preferred_element_type=F32)
    for q in range(SEQ):
        ns_m[q] = nsf[pl.ds(q, PROP, stride=SEQ), :][:, 0:8].astype(BF16)

    dt = softplus(wide + bias)
    sbuf[...] = -rate * dt
    run = jnp.zeros((SEQ, 512), F32)
    lb[0:12, :] = jnp.zeros((12, 512), F32)
    dtb[0:12, :] = jnp.zeros((12, 512), F32)
    xb[0:12, :] = jnp.zeros((12, 512), F32)
    bb[0:12, :] = jnp.zeros((12, 128), F32)
    for t in range(PROP):
        run = run + sbuf[SEQ * t : SEQ * t + SEQ, :]
        lb[12 + SEQ * t : 16 + SEQ * t, :] = run
    dtb[12:28, :] = dt
    logs = lb[12:28, :]
    for j in range(PROP):
        lo = 12 - SEQ * j
        dj[j] = jnp.exp(logs - lb[lo : lo + ROWS, :]) * dtb[lo : lo + ROWS, :]

    eight = (
        lax.broadcasted_iota(jnp.int32, (8, 512), 0)
        == lax.broadcasted_iota(jnp.int32, (8, 512), 1) // 64
    )
    eight = jnp.where(eight, 1.0, 0.0).astype(BF16)
    for q in range(SEQ):
        stp[PROP * q : PROP * q + PROP, :] = jnp.dot(
            ps_m[q], eight, preferred_element_type=F32
        )
    steps = jnp.dot(swap, stp[...].astype(BF16), preferred_element_type=F32)
    pd = softplus(steps + bias)

    def taken(shape):
        seq = lax.broadcasted_iota(jnp.int32, shape, 0) % SEQ
        count = jnp.full(shape, taken_m[0], jnp.int32)
        for q in range(1, SEQ):
            count = jnp.where(seq == q, taken_m[q], count)
        return count

    live = lax.broadcasted_iota(jnp.int32, (ROWS, 512), 0) // SEQ < taken((ROWS, 512))
    sbuf[...] = jnp.where(live, -rate * pd, 0.0)
    pls = [sbuf[SEQ * s : SEQ * s + SEQ, :] for s in range(PROP)]
    tails = [None] * PROP
    run = jnp.zeros((SEQ, 512), F32)
    for s in reversed(range(PROP)):
        tails[s] = run
        run = run + pls[s]
    kept = jnp.exp(run)
    for s in range(PROP):
        stp[SEQ * s : SEQ * s + SEQ, :] = jnp.exp(tails[s])
    ubuf[...] = jnp.where(live, stp[...] * pd, 0.0) * silu(conv(ppv, cv_m))
    bbuf[...] = silu(conv(ppb, cb_m))

    def window(pp, rr, width):
        count = taken((12, width))
        first = pp[SEQ : SEQ + 12, :]
        for a in range(2, PROP + 1):
            first = jnp.where(count == a, pp[SEQ * a : SEQ * a + 12, :], first)
        rr[0:12, :] = first

    window(ppv, rrv, 512)
    window(ppb, rrb, 128)
    window(ppc, rrc, 128)

    rest = pl.ds(0, ROWS * (N - 1))

    def others(me):
        return [i + jnp.where(me <= i, 1, 0).astype(jnp.int32) for i in range(N - 1)]

    def sums_y():
        arrived(T2Z, az.at[rest, :])
        spread_end(ring_z)
        pz[...] = jnp.dot(az[...], wz[...], preferred_element_type=F32).astype(BF16)
        for yy in others(y):
            send(RSZ, pz.at[at(yy, ROWS), :], rsz.at[y], z * N + yy, tp)

    def sums_z():
        arrived(T2Y, ay.at[rest, :])
        spread_end(ring_y)
        py[...] = jnp.dot(ay[...], wy[...], preferred_element_type=F32).astype(BF16)
        for zz in others(z):
            send(RSY, py.at[at(zz, ROWS), :], rsy.at[z], zz * N + y, tp)

    @pl.when(z < 4)
    def _():
        sums_y()
        sums_z()
        spread_own((ring_o,))
        spread_far((ring_o,))

    @pl.when(z >= 4)
    def _():
        sums_z()
        spread_own((ring_o,))
        spread_far((ring_o,))
        sums_y()

    rsy[z] = py[at(z, ROWS), :]
    rsz[y] = pz[at(y, ROWS), :]

    seq = lax.broadcasted_iota(jnp.int32, (ROWS, 512), 0) % SEQ
    for q in range(SEQ):
        u = jnp.where(seq == q, ubuf[...], 0.0)
        grown = lax.dot_general(u, bbuf[...], TN, precision=HIGHEST, preferred_element_type=F32)
        for h in range(8):
            lo = 512 * q + 64 * h
            old = jnp.broadcast_to(kept[q : q + 1, 64 * h : 64 * h + 1], (64, 128))
            new = old * base_m[lo : lo + 64, :] + grown[64 * h : 64 * h + 64, :]
            root_m[lo : lo + 64, :] = new
            rootb[lo : lo + 64, :] = new.astype(BF16)

    @pl.when(z >= 4)
    def _():
        spread_on((ring_o,))

    arrived(RSY, rsy.at[pl.ds(0, N - 1)])
    arrived(RSZ, rsz.at[pl.ds(0, N - 1)])

    def summed(ref, lo, hi):
        total = ref[0, :, lo:hi].astype(F32)
        for s in range(1, N):
            total = total + ref[s, :, lo:hi].astype(F32)
        return total.astype(BF16).astype(F32)

    rrv[12:28, :] = summed(rsy, 0, 512)
    rrb[12:28, :] = summed(rsy, 512, 640)
    rrc[12:28, :] = summed(rsz, 512, 640)
    gate = summed(rsz, 0, 512)
    x = silu(conv(rrv, cv_m))
    b = silu(conv(rrb, cb_m))
    c = silu(conv(rrc, cc_m))
    xb[12:28, :] = x
    bb[12:28, :] = b
    c16 = c.astype(BF16)
    carried = jnp.zeros((ROWS, 512), F32)
    for q in range(SEQ):
        one = lax.dot_general(
            c16, rootb[512 * q : 512 * q + 512, :], NT, preferred_element_type=F32
        )
        carried = jnp.where(seq == q, one, carried)
    out = jnp.exp(logs) * carried + skip * x
    for j in range(PROP):
        lo = 12 - SEQ * j
        score = jnp.sum(c * bb[lo : lo + ROWS, :], axis=-1, keepdims=True)
        out = out + score * dj[j] * xb[lo : lo + ROWS, :]
    g = out * silu(gate)
    g = g * lax.rsqrt(jnp.mean(g * g, axis=-1, keepdims=True) + EPSILON)
    nrg[at(z, ROWS), :] = (g * og_m[...]).astype(BF16)
    slot = LATE + lax.div(z, 2)
    for d in ORDER:
        copy(O1, slot, nrg.at[at(z, ROWS), :], nrg.at[at(z, ROWS), :], over(d), tp).start()

    @pl.when(z < 4)
    def _():
        spread_on((ring_o,))

    for r in range(PAST):
        nv_m[r] = rrv[SEQ * r : SEQ * r + SEQ, :].astype(BF16)
        nb_m[r] = rrb[SEQ * r : SEQ * r + SEQ, :].astype(BF16)
        nc_m[r] = rrc[SEQ * r : SEQ * r + SEQ, :].astype(BF16)

    spread_end(ring_o)
    for pair in range(4):
        near = lax.div(z, 2) == pair
        sem = LATE + pair

        @pl.when(near)
        def _():
            one = nrg.at[pl.ds(0, ROWS), :]
            copy(O1, sem, one, one, kv, tp).wait_recv()

        @pl.when(jnp.logical_not(near))
        def _():
            two = nrg.at[pl.ds(0, 2 * ROWS), :]
            copy(O1, sem, two, two, kv, tp).wait_recv()

        part = pl.ds(32 * pair, 32)
        po[part, :] = lax.dot_general(
            nrg[part, :], owg[...], NT, preferred_element_type=F32
        ).astype(BF16)
        for zz in (2 * pair, 2 * pair + 1):
            local = jnp.logical_and(z == zz, tp == zz)

            @pl.when(jnp.logical_not(local))
            def _():
                send(O2, po.at[pl.ds(ROWS * zz, ROWS), :], osum.at[tp], zz * N + y, z)

            @pl.when(local)
            def _():
                osum[tp] = po[ROWS * zz : ROWS * zz + ROWS, :]

    @pl.when(z != tp)
    def _():
        arrived(O2, osum)

    @pl.when(z == tp)
    def _():
        arrived(O2, osum.at[pl.ds(0, N - 1)])

    total = osum[0].astype(F32)
    for t in range(1, N):
        total = total + osum[t].astype(F32)
    for i in range(2):
        mf[i] = total[:, 128 * i : 128 * i + 128]
        for q in range(SEQ):
            mixed_m[q, :, 128 * i : 128 * i + 128] = mf.at[i][
                pl.ds(q, PROP, stride=SEQ), :
            ].astype(BF16)

    gone(T1, xall.at[pl.ds(0, N - 1)])
    gone(T2Y, ay.at[rest, :])
    gone(T2Z, az.at[rest, :])
    gone(WY, wy.at[pl.ds(0, 224), :])
    gone(WZ, wz.at[pl.ds(0, 224), :])
    gone(RSY, rsy.at[pl.ds(0, N - 1)])
    gone(RSZ, rsz.at[pl.ds(0, N - 1)])
    gone(OW, owg.at[pl.ds(0, 224), :])
    gone(O1, nrg.at[rest, :])

    @pl.when(z != tp)
    def _():
        gone(O2, osum)

    @pl.when(z == tp)
    def _():
        gone(O2, osum.at[pl.ds(0, N - 1)])


def finish(*refs):
    ins, outs, sem = refs[:6], refs[6:12], refs[12]
    pairs = [(s, d) for i, (s, d) in enumerate(zip(ins, outs)) if i != 1]
    pairs += [(ins[1].at[part], outs[1].at[part]) for part in (pl.ds(512 * i, 512) for i in range(4))]
    copies = [pltpu.make_async_copy(s, d, sem.at[i]) for i, (s, d) in enumerate(pairs)]
    for c in copies:
        c.start()
    for c in copies:
        c.wait()


def on_device(
    tokens, input_gain, gate_weight, value_weight, write_weight, read_weight, step_weight,
    conv_value, conv_write, conv_read, step_bias, decay_log, skip_gain, output_gain,
    out_weight, base_state, past_value, past_write, past_read, past_step, accepted,
):
    vmem = pltpu.VMEM
    ops = (
        tokens, input_gain[None, :], gate_weight, value_weight, write_weight, read_weight,
        step_weight.T, conv_value, conv_write, conv_read, step_bias[None, :],
        decay_log[None, :], skip_gain[None, :], output_gain[None, :], out_weight.T,
        base_state.reshape(2048, 128), past_value.transpose(1, 0, 2),
        past_write.transpose(1, 0, 2), past_read.transpose(1, 0, 2), past_step, accepted,
    )
    out_shapes = [
        ((SEQ, PROP, 256), BF16), ((2048, 128), F32), ((PAST, SEQ, 512), BF16),
        ((PAST, SEQ, 128), BF16), ((PAST, SEQ, 128), BF16), ((SEQ, PROP, 8), BF16),
    ]
    scratch = [
        vmem((1, 2048), F32), vmem((64, 2048), BF16), vmem((4, 512), F32), vmem((4, 128), F32),
        vmem((4, 128), F32), vmem((1, 8), F32), vmem((1, 8), F32), vmem((1, 8), F32),
        vmem((1, 512), F32), vmem((2048, 128), F32), vmem((PAST, SEQ, 512), BF16),
        vmem((PAST, SEQ, 128), BF16), vmem((PAST, SEQ, 128), BF16), vmem((SEQ, PROP, 8), BF16),
        vmem((SEQ, PROP, 256), BF16),
        vmem((N, ROWS, 256), BF16), vmem((N, ROWS, 256), BF16), vmem((N, ROWS, 256), BF16),
        vmem((128, 256), BF16), vmem((128, 256), BF16), vmem((256, 640), BF16),
        vmem((256, 640), BF16), vmem((128, 640), BF16), vmem((128, 640), BF16),
        vmem((N, ROWS, 640), BF16), vmem((N, ROWS, 640), BF16), vmem((256, 512), BF16),
        vmem((128, 512), BF16), vmem((128, 256), BF16), vmem((N, ROWS, 256), BF16),
        vmem((ROWS, 256), F32), vmem((28, 512), F32), vmem((28, 128), F32), vmem((28, 128), F32),
        vmem((28, 512), F32), vmem((28, 128), F32), vmem((28, 128), F32), vmem((ROWS, 512), F32),
        vmem((ROWS, 512), F32), vmem((ROWS, 512), F32), vmem((ROWS, 128), F32),
        vmem((28, 512), F32), vmem((28, 128), F32), vmem((28, 512), F32), vmem((28, 512), F32),
        vmem((PROP, ROWS, 512), F32), vmem((2048, 128), BF16), vmem((2, ROWS, 128), F32),
        vmem((ROWS, 128), F32),
        pltpu.SMEM((SEQ,), jnp.int32),
        pltpu.SemaphoreType.DMA((9,)),
        pltpu.SemaphoreType.DMA((10,)),
        pltpu.SemaphoreType.DMA((26,)),
        pltpu.SemaphoreType.REGULAR,
    ]
    held = pl.pallas_call(
        body,
        out_shape=[vmem(shape, dtype) for shape, dtype in out_shapes],
        in_specs=[pl.BlockSpec(memory_space=pl.ANY)] * 21,
        out_specs=[pl.BlockSpec(memory_space=vmem)] * 6,
        scratch_shapes=scratch,
        compiler_params=pltpu.CompilerParams(collective_id=0, has_side_effects=True),
        name="mixer",
    )(*ops)
    mixed, root, nv, nb, nc, ns = pl.pallas_call(
        finish,
        out_shape=[jax.ShapeDtypeStruct(shape, dtype) for shape, dtype in out_shapes],
        in_specs=[pl.BlockSpec(memory_space=vmem)] * 6,
        out_specs=[pl.BlockSpec(memory_space=pl.ANY)] * 6,
        scratch_shapes=[pltpu.SemaphoreType.DMA((9,))],
        name="finish",
    )(*(pltpu.with_memory_space_constraint(h, vmem) for h in held))
    return (
        mixed, root.reshape(base_state.shape), nv.transpose(1, 0, 2), nb.transpose(1, 0, 2),
        nc.transpose(1, 0, 2), ns,
    )


def solution(mesh):
    return jax.shard_map(
        on_device,
        mesh=mesh,
        in_specs=(
            P("kv", None, "tp"), P(), P("kv", "tp"), P("kv", "tp"), P("kv", "tp"), P("kv", "tp"),
            P(), P(None, "tp"), P(None, "tp"), P(None, "tp"), P("tp"), P("tp"), P("tp"), P("tp"),
            P("tp", "kv"), P("kv", "tp", None, None), P("kv", None, "tp"), P("kv", None, "tp"),
            P("kv", None, "tp"), P("kv", None, "tp"), P("kv"),
        ),
        out_specs=(
            P("kv", None, "tp"), P("kv", "tp", None, None), P("kv", None, "tp"),
            P("kv", None, "tp"), P("kv", None, "tp"), P("kv", None, "tp"),
        ),
        check_vma=False,
    )
```

```python
import jax
import jax.numpy as jnp
from jax import lax
from jax.experimental import pallas as pl
from jax.experimental.pallas import tpu as pltpu
from jax.sharding import PartitionSpec as P

F32 = jnp.float32
BF16 = jnp.bfloat16
MESH = pl.DeviceIdType.MESH
EPSILON = 1e-06
HIGHEST = lax.Precision.HIGHEST

N = 8
SEQ = 4
PROP = 4
ROWS = SEQ * PROP
CONV = 4
PAST = 7
NT = (((1,), (1,)), ((), ()))
TN = (((0,), (0,)), ((), ()))
ORDER = (4, 3, 5, 2, 6, 1, 7)

T1, T2Y, T2Z, WY, WZ, RSY, RSZ, OW, O1, O2 = range(10)
LATE = 22


def silu(v):
    return v / (1.0 + jnp.exp(-v))


def softplus(v):
    return jnp.maximum(v, 0.0) + jnp.log1p(jnp.exp(-jnp.abs(v)))


def conv(buf, taps, at=0):
    total = taps[0:1, :] * buf[at : at + ROWS, :]
    for k in range(1, CONV):
        total = total + taps[k : k + 1, :] * buf[at + SEQ * k : at + SEQ * k + ROWS, :]
    return total


def body(
    tokens, input_gain, gate_w, value_w, write_w, read_w, step_w,
    conv_v, conv_b, conv_c, step_bias, decay_log, skip_gain, output_gain,
    out_w, base, past_v, past_b, past_c, past_s, accepted,
    mixed_m, root_m, nv_m, nb_m, nc_m, ns_m,
    gain_m, stepw_m, cv_m, cb_m, cc_m, bias_m, decay_m, skip_m, og_m,
    base_m, pv_m, pb_m, pc_m, ps_m, tok_m,
    xall, nrm, npk, ay, az, wy, wz, py, pz, rsy, rsz, owg, nrg, po, osum,
    xf, ppv, ppb, ppc, rrv, rrb, rrc, stp, sbuf, ubuf, bbuf, xb, bb, lb, dtb, dj, rootb, mf, nsf,
    taken_m,
    in_sem, send_sem, recv_sem, hello,
):
    kv = lax.axis_index("kv")
    tp = lax.axis_index("tp")
    z = lax.div(kv, N)
    y = lax.rem(kv, N)

    def at(rows, count):
        return pl.ds(pl.multiple_of(rows * count, count), count)

    def up(d):
        return z * N + lax.rem(y + d, N)

    def over(d):
        return (lax.rem(z + d, N)) * N + y

    groups = (
        (
            (value_w, wy.at[at(y, 32), pl.ds(0, 512)]),
            (write_w, wy.at[at(y, 32), pl.ds(512, 128)]),
            (gate_w, wz.at[at(z, 32), pl.ds(0, 512)]),
            (read_w, wz.at[at(z, 32), pl.ds(512, 128)]),
            (out_w, owg.at[at(y, 32), :]),
            (tokens, tok_m),
        ),
        (
            (input_gain, gain_m),
            (past_v, pv_m),
            (past_b, pb_m),
            (past_c, pc_m),
            (conv_v, cv_m),
            (conv_b, cb_m),
            (conv_c, cc_m),
            (output_gain, og_m),
        ),
        ((past_s, ps_m),),
        ((step_bias, bias_m),),
        ((decay_log, decay_m),),
        ((skip_gain, skip_m),),
        ((accepted, taken_m),),
        ((step_w, stepw_m),),
        ((base, base_m),),
    )
    for i, group in enumerate(groups):
        for source, target in group:
            pltpu.make_async_copy(source, target, in_sem.at[i]).start()

    def loaded(i, ref=None):
        if ref is None:
            pltpu.make_async_copy(*groups[i][0], in_sem.at[i]).wait()
        else:
            pltpu.make_async_copy(ref, ref, in_sem.at[i]).wait()

    barrier = pltpu.get_barrier_semaphore()

    def tell(k, t):
        pl.semaphore_signal(barrier, inc=1, device_id=(k, t), device_id_type=MESH)

    for d in range(1, N):
        tell(kv, lax.rem(tp + d, N))
    for d in (1, 7, 2, 6):
        tell(up(d), tp)
        tell(over(d), tp)

    loaded(0, wy.at[pl.ds(0, 96), :])
    to = lax.broadcasted_iota(jnp.int32, (ROWS, ROWS), 0)
    by = lax.broadcasted_iota(jnp.int32, (ROWS, ROWS), 1)
    swap = jnp.where((to % SEQ) * PROP + to // SEQ == by, 1.0, 0.0).astype(BF16)
    for q in range(SEQ):
        xf[PROP * q : PROP * q + PROP, :] = tok_m[q].astype(F32)
    xall[tp] = jnp.dot(swap, xf[...].astype(BF16), preferred_element_type=F32).astype(BF16)
    pl.semaphore_wait(barrier, N - 1 + 8)
    for d in (2, 6):
        pl.semaphore_signal(hello, inc=1, device_id=(up(d), tp), device_id_type=MESH)
        pl.semaphore_signal(hello, inc=1, device_id=(over(d), tp), device_id_type=MESH)

    def copy(phase, slot, src, dst, k, t):
        return pltpu.make_async_remote_copy(
            src_ref=src, dst_ref=dst, send_sem=send_sem.at[1 if phase in (OW, O1, O2) else 0],
            recv_sem=recv_sem.at[slot],
            device_id=(k, t), device_id_type=MESH,
        )

    def send(phase, src, dst, k, t):
        copy(phase, phase, src, dst, k, t).start()

    def arrived(phase, ref):
        copy(phase, phase, ref, ref, kv, tp).wait_recv()

    def gone(phase, ref):
        copy(phase, phase, ref, ref, kv, tp).wait_send()

    def slab(ref, owner, h):
        return ref.at[pl.ds(pl.multiple_of(owner * 32 + 16 * h, 16), 16), :]

    def pass_slab(phase, slot, ref, owner, h, k):
        copy(phase, slot, slab(ref, owner, h), slab(ref, owner, h), k, tp).start()

    def early(first, h, side):
        return first + 2 * h + side

    def spread_own(rings, steps=((2, 6), (1, 7))):
        for ds in steps:
            for h in range(2):
                for side, d in enumerate(ds):
                    for phase, first, ref, me, dev in rings:
                        slot = early(first, h, side) if d in (2, 6) else phase
                        pass_slab(phase, slot, ref, me, h, dev(d))

    def spread_far(rings):
        for h in range(2):
            for phase, first, ref, me, dev in rings:
                pass_slab(phase, phase, ref, me, h, dev(4))

    def spread_on(rings):
        for h in range(2):
            for side, (back_two, one) in enumerate(((6, 1), (2, 7))):
                for phase, first, ref, me, dev in rings:
                    owner = lax.rem(me + back_two, N)
                    part = slab(ref, owner, h)
                    copy(phase, early(first, h, side), part, part, kv, tp).wait_recv()
                    pass_slab(phase, phase, ref, owner, h, dev(one))

    def spread_end(ring):
        arrived(ring[0], ring[2].at[pl.ds(0, 160), :])

    ring_y = (WY, 10, wy, y, up)
    ring_z = (WZ, 14, wz, z, over)
    ring_o = (OW, 18, owg, y, up)

    for d in range(1, N):
        send(T1, xall.at[tp], xall.at[tp], kv, lax.rem(tp + d, N))
    spread_own((ring_y, ring_z))

    loaded(1, base_m.at[pl.ds(0, 128), :])
    for i in range(2, 9):
        loaded(i)
    for r in range(PAST):
        ppv[SEQ * r : SEQ * r + SEQ, :] = pv_m[r].astype(F32)
        ppb[SEQ * r : SEQ * r + SEQ, :] = pb_m[r].astype(F32)
        ppc[SEQ * r : SEQ * r + SEQ, :] = pc_m[r].astype(F32)

    pl.semaphore_wait(hello, 4)
    spread_far((ring_y, ring_z))

    arrived(T1, xall.at[pl.ds(0, N - 1)])
    blocks = [xall[t].astype(F32) for t in range(N)]
    square = blocks[0] * blocks[0]
    for t in range(1, N):
        square = square + blocks[t] * blocks[t]
    scale = lax.rsqrt(jnp.sum(square, axis=-1, keepdims=True) * (1.0 / 2048) + EPSILON)
    normed = []
    for t in range(N):
        block = (blocks[t] * scale * gain_m[:, 256 * t : 256 * t + 256]).astype(BF16)
        nrm[t] = block
        normed.append(block.astype(F32))
    ay[at(z, ROWS), :] = nrm[z]
    for d in ORDER:
        zz = lax.rem(z + d, N)
        send(T2Y, nrm.at[zz], ay.at[at(z, ROWS), :], over(d), tp)
    lane = lax.broadcasted_iota(jnp.int32, (ROWS, 128), 1) // 32
    for yy in range(N):
        for half in range(2):
            tile = None
            for i in range(4):
                shift = (32 * i - 32 * (yy % 4)) % 128
                start = 128 * (yy // 4)
                piece = normed[4 * half + i][:, start : start + 128]
                if shift:
                    piece = pltpu.roll(piece, shift, 1)
                tile = piece if tile is None else jnp.where(lane == i, piece, tile)
            npk[yy, :, 128 * half : 128 * half + 128] = tile.astype(BF16)
    az[at(y, ROWS), :] = npk[y]
    for d in ORDER:
        yy = lax.rem(y + d, N)
        send(T2Z, npk.at[yy], az.at[at(y, ROWS), :], up(d), tp)
    spread_on((ring_y, ring_z))
    spread_own((ring_o,), ((2, 6),))

    head = lax.broadcasted_iota(jnp.int32, (1, 512), 1) // 64

    def spread(ref):
        row = jnp.zeros((1, 512), F32)
        for h in range(8):
            row = jnp.where(head == h, ref[0:1, h : h + 1], row)
        return row

    bias = spread(bias_m)
    rate = jnp.exp(spread(decay_m))
    skip = spread(skip_m)
    step = jnp.zeros((ROWS, 64), F32)
    for t in range(N):
        weight = stepw_m[:, 256 * t : 256 * t + 256]
        step = step + lax.dot_general(nrm[t], weight, NT, preferred_element_type=F32)
    step16 = step.astype(BF16)
    row64 = lax.broadcasted_iota(jnp.int32, (64, 512), 0)
    own64 = (row64 - 8 * tp == lax.broadcasted_iota(jnp.int32, (64, 512), 1) // 64)
    wide = jnp.dot(step16, jnp.where(own64, 1.0, 0.0).astype(BF16), preferred_element_type=F32)
    row64 = lax.broadcasted_iota(jnp.int32, (64, 128), 0)
    pick = (row64 - 8 * tp == lax.broadcasted_iota(jnp.int32, (64, 128), 1))
    nsf[...] = jnp.dot(step16, jnp.where(pick, 1.0, 0.0).astype(BF16), preferred_element_type=F32)
    for q in range(SEQ):
        ns_m[q] = nsf[pl.ds(q, PROP, stride=SEQ), :][:, 0:8].astype(BF16)

    dt = softplus(wide + bias)
    sbuf[...] = -rate * dt
    run = jnp.zeros((SEQ, 512), F32)
    lb[0:12, :] = jnp.zeros((12, 512), F32)
    dtb[0:12, :] = jnp.zeros((12, 512), F32)
    xb[0:12, :] = jnp.zeros((12, 512), F32)
    bb[0:12, :] = jnp.zeros((12, 128), F32)
    for t in range(PROP):
        run = run + sbuf[SEQ * t : SEQ * t + SEQ, :]
        lb[12 + SEQ * t : 16 + SEQ * t, :] = run
    dtb[12:28, :] = dt
    logs = lb[12:28, :]
    for j in range(PROP):
        lo = 12 - SEQ * j
        dj[j] = jnp.exp(logs - lb[lo : lo + ROWS, :]) * dtb[lo : lo + ROWS, :]

    eight = (
        lax.broadcasted_iota(jnp.int32, (8, 512), 0)
        == lax.broadcasted_iota(jnp.int32, (8, 512), 1) // 64
    )
    eight = jnp.where(eight, 1.0, 0.0).astype(BF16)
    for q in range(SEQ):
        stp[PROP * q : PROP * q + PROP, :] = jnp.dot(
            ps_m[q], eight, preferred_element_type=F32
        )
    steps = jnp.dot(swap, stp[...].astype(BF16), preferred_element_type=F32)
    pd = softplus(steps + bias)

    def taken(shape):
        seq = lax.broadcasted_iota(jnp.int32, shape, 0) % SEQ
        count = jnp.full(shape, taken_m[0], jnp.int32)
        for q in range(1, SEQ):
            count = jnp.where(seq == q, taken_m[q], count)
        return count

    live = lax.broadcasted_iota(jnp.int32, (ROWS, 512), 0) // SEQ < taken((ROWS, 512))
    sbuf[...] = jnp.where(live, -rate * pd, 0.0)
    pls = [sbuf[SEQ * s : SEQ * s + SEQ, :] for s in range(PROP)]
    tails = [None] * PROP
    run = jnp.zeros((SEQ, 512), F32)
    for s in reversed(range(PROP)):
        tails[s] = run
        run = run + pls[s]
    kept = jnp.exp(run)
    for s in range(PROP):
        stp[SEQ * s : SEQ * s + SEQ, :] = jnp.exp(tails[s])
    ubuf[...] = jnp.where(live, stp[...] * pd, 0.0) * silu(conv(ppv, cv_m))
    bbuf[...] = silu(conv(ppb, cb_m))

    def window(pp, rr, width):
        count = taken((12, width))
        first = pp[SEQ : SEQ + 12, :]
        for a in range(2, PROP + 1):
            first = jnp.where(count == a, pp[SEQ * a : SEQ * a + 12, :], first)
        rr[0:12, :] = first

    window(ppv, rrv, 512)
    window(ppb, rrb, 128)
    window(ppc, rrc, 128)

    rest = pl.ds(0, ROWS * (N - 1))

    def others(me):
        return [i + jnp.where(me <= i, 1, 0).astype(jnp.int32) for i in range(N - 1)]

    def sums_y():
        arrived(T2Z, az.at[rest, :])
        spread_end(ring_z)
        pz[...] = jnp.dot(az[...], wz[...], preferred_element_type=F32).astype(BF16)
        for yy in others(y):
            copy(RSZ, RSY, pz.at[at(yy, ROWS), :], rsz.at[y], z * N + yy, tp).start()

    def sums_z():
        arrived(T2Y, ay.at[rest, :])
        spread_end(ring_y)
        py[...] = jnp.dot(ay[...], wy[...], preferred_element_type=F32).astype(BF16)
        for zz in others(z):
            send(RSY, py.at[at(zz, ROWS), :], rsy.at[z], zz * N + y, tp)

    @pl.when(z < 4)
    def _():
        sums_y()
        spread_own((ring_o,), ((1, 7),))
        spread_far((ring_o,))
        sums_z()

    @pl.when(z >= 4)
    def _():
        sums_z()
        sums_y()
        spread_own((ring_o,), ((1, 7),))
        spread_far((ring_o,))

    rsy[z] = py[at(z, ROWS), :]
    rsz[y] = pz[at(y, ROWS), :]

    seq = lax.broadcasted_iota(jnp.int32, (ROWS, 512), 0) % SEQ
    for q in range(SEQ):
        u = jnp.where(seq == q, ubuf[...], 0.0)
        grown = lax.dot_general(u, bbuf[...], TN, precision=HIGHEST, preferred_element_type=F32)
        for h in range(8):
            lo = 512 * q + 64 * h
            old = jnp.broadcast_to(kept[q : q + 1, 64 * h : 64 * h + 1], (64, 128))
            new = old * base_m[lo : lo + 64, :] + grown[64 * h : 64 * h + 64, :]
            root_m[lo : lo + 64, :] = new
            rootb[lo : lo + 64, :] = new.astype(BF16)

    spread_on((ring_o,))

    arrived(RSY, wy.at[pl.ds(0, 224), :])

    def summed(ref, lo, hi):
        total = ref[0, :, lo:hi].astype(F32)
        for s in range(1, N):
            total = total + ref[s, :, lo:hi].astype(F32)
        return total.astype(BF16).astype(F32)

    rrv[12:28, :] = summed(rsy, 0, 512)
    rrb[12:28, :] = summed(rsy, 512, 640)
    rrc[12:28, :] = summed(rsz, 512, 640)
    gate = summed(rsz, 0, 512)
    x = silu(conv(rrv, cv_m))
    b = silu(conv(rrb, cb_m))
    c = silu(conv(rrc, cc_m))
    xb[12:28, :] = x
    bb[12:28, :] = b
    c16 = c.astype(BF16)
    carried = jnp.zeros((ROWS, 512), F32)
    for q in range(SEQ):
        one = lax.dot_general(
            c16, rootb[512 * q : 512 * q + 512, :], NT, preferred_element_type=F32
        )
        carried = jnp.where(seq == q, one, carried)
    out = jnp.exp(logs) * carried + skip * x
    for j in range(PROP):
        lo = 12 - SEQ * j
        score = jnp.sum(c * bb[lo : lo + ROWS, :], axis=-1, keepdims=True)
        out = out + score * dj[j] * xb[lo : lo + ROWS, :]
    g = out * silu(gate)
    g = g * lax.rsqrt(jnp.mean(g * g, axis=-1, keepdims=True) + EPSILON)
    nrg[at(z, ROWS), :] = (g * og_m[...]).astype(BF16)
    slot = LATE + jnp.where(z < 2, z, lax.div(z, 2) + 1).astype(jnp.int32)
    for d in ORDER:
        copy(O1, slot, nrg.at[at(z, ROWS), :], nrg.at[at(z, ROWS), :], over(d), tp).start()
    for r in range(PAST):
        nv_m[r] = rrv[SEQ * r : SEQ * r + SEQ, :].astype(BF16)
        nb_m[r] = rrb[SEQ * r : SEQ * r + SEQ, :].astype(BF16)
        nc_m[r] = rrc[SEQ * r : SEQ * r + SEQ, :].astype(BF16)

    spread_end(ring_o)
    for i, (low, high) in enumerate(((0, 1), (1, 2), (2, 4), (4, 6), (6, 8))):
        mine = jnp.logical_and(z >= low, z < high)
        sem = LATE + i

        def landed(count):
            if count:
                some = nrg.at[pl.ds(0, count * ROWS), :]
                copy(O1, sem, some, some, kv, tp).wait_recv()

        if high - low > 1:

            @pl.when(mine)
            def _():
                landed(high - low - 1)

        @pl.when(jnp.logical_not(mine))
        def _():
            landed(high - low)

        part = pl.ds(ROWS * low, ROWS * (high - low))
        po[part, :] = lax.dot_general(
            nrg[part, :], owg[...], NT, preferred_element_type=F32
        ).astype(BF16)
        for zz in range(low, high):
            local = jnp.logical_and(z == zz, tp == zz)

            @pl.when(jnp.logical_not(local))
            def _():
                send(O2, po.at[pl.ds(ROWS * zz, ROWS), :], osum.at[tp], zz * N + y, z)

            @pl.when(local)
            def _():
                osum[tp] = po[ROWS * zz : ROWS * zz + ROWS, :]

    @pl.when(z != tp)
    def _():
        arrived(O2, osum)

    @pl.when(z == tp)
    def _():
        arrived(O2, osum.at[pl.ds(0, N - 1)])

    total = osum[0].astype(F32)
    for t in range(1, N):
        total = total + osum[t].astype(F32)
    for i in range(2):
        mf[i] = total[:, 128 * i : 128 * i + 128]
        for q in range(SEQ):
            mixed_m[q, :, 128 * i : 128 * i + 128] = mf.at[i][
                pl.ds(q, PROP, stride=SEQ), :
            ].astype(BF16)

    gone(T1, base_m.at[pl.ds(0, 2016), :])

    @pl.when(z != tp)
    def _():
        gone(O2, base_m.at[pl.ds(0, 800), :])

    @pl.when(z == tp)
    def _():
        gone(O2, base_m.at[pl.ds(0, 784), :])


def finish(*refs):
    ins, outs, sem = refs[:6], refs[6:12], refs[12]
    pairs = [(s, d) for i, (s, d) in enumerate(zip(ins, outs)) if i != 1]
    pairs += [(ins[1].at[part], outs[1].at[part]) for part in (pl.ds(512 * i, 512) for i in range(4))]
    copies = [pltpu.make_async_copy(s, d, sem.at[i]) for i, (s, d) in enumerate(pairs)]
    for c in copies:
        c.start()
    for c in copies:
        c.wait()


def on_device(
    tokens, input_gain, gate_weight, value_weight, write_weight, read_weight, step_weight,
    conv_value, conv_write, conv_read, step_bias, decay_log, skip_gain, output_gain,
    out_weight, base_state, past_value, past_write, past_read, past_step, accepted,
):
    vmem = pltpu.VMEM
    ops = (
        tokens, input_gain[None, :], gate_weight, value_weight, write_weight, read_weight,
        step_weight.T, conv_value, conv_write, conv_read, step_bias[None, :],
        decay_log[None, :], skip_gain[None, :], output_gain[None, :], out_weight.T,
        base_state.reshape(2048, 128), past_value.transpose(1, 0, 2),
        past_write.transpose(1, 0, 2), past_read.transpose(1, 0, 2), past_step, accepted,
    )
    out_shapes = [
        ((SEQ, PROP, 256), BF16), ((2048, 128), F32), ((PAST, SEQ, 512), BF16),
        ((PAST, SEQ, 128), BF16), ((PAST, SEQ, 128), BF16), ((SEQ, PROP, 8), BF16),
    ]
    scratch = [
        vmem((1, 2048), F32), vmem((64, 2048), BF16), vmem((4, 512), F32), vmem((4, 128), F32),
        vmem((4, 128), F32), vmem((1, 8), F32), vmem((1, 8), F32), vmem((1, 8), F32),
        vmem((1, 512), F32), vmem((2048, 128), F32), vmem((PAST, SEQ, 512), BF16),
        vmem((PAST, SEQ, 128), BF16), vmem((PAST, SEQ, 128), BF16), vmem((SEQ, PROP, 8), BF16),
        vmem((SEQ, PROP, 256), BF16),
        vmem((N, ROWS, 256), BF16), vmem((N, ROWS, 256), BF16), vmem((N, ROWS, 256), BF16),
        vmem((128, 256), BF16), vmem((128, 256), BF16), vmem((256, 640), BF16),
        vmem((256, 640), BF16), vmem((128, 640), BF16), vmem((128, 640), BF16),
        vmem((N, ROWS, 640), BF16), vmem((N, ROWS, 640), BF16), vmem((256, 512), BF16),
        vmem((128, 512), BF16), vmem((128, 256), BF16), vmem((N, ROWS, 256), BF16),
        vmem((ROWS, 256), F32), vmem((28, 512), F32), vmem((28, 128), F32), vmem((28, 128), F32),
        vmem((28, 512), F32), vmem((28, 128), F32), vmem((28, 128), F32), vmem((ROWS, 512), F32),
        vmem((ROWS, 512), F32), vmem((ROWS, 512), F32), vmem((ROWS, 128), F32),
        vmem((28, 512), F32), vmem((28, 128), F32), vmem((28, 512), F32), vmem((28, 512), F32),
        vmem((PROP, ROWS, 512), F32), vmem((2048, 128), BF16), vmem((2, ROWS, 128), F32),
        vmem((ROWS, 128), F32),
        pltpu.SMEM((SEQ,), jnp.int32),
        pltpu.SemaphoreType.DMA((9,)),
        pltpu.SemaphoreType.DMA((2,)),
        pltpu.SemaphoreType.DMA((27,)),
        pltpu.SemaphoreType.REGULAR,
    ]
    held = pl.pallas_call(
        body,
        out_shape=[vmem(shape, dtype) for shape, dtype in out_shapes],
        in_specs=[pl.BlockSpec(memory_space=pl.ANY)] * 21,
        out_specs=[pl.BlockSpec(memory_space=vmem)] * 6,
        scratch_shapes=scratch,
        compiler_params=pltpu.CompilerParams(collective_id=0, has_side_effects=True),
        name="mixer",
    )(*ops)
    mixed, root, nv, nb, nc, ns = pl.pallas_call(
        finish,
        out_shape=[jax.ShapeDtypeStruct(shape, dtype) for shape, dtype in out_shapes],
        in_specs=[pl.BlockSpec(memory_space=vmem)] * 6,
        out_specs=[pl.BlockSpec(memory_space=pl.ANY)] * 6,
        scratch_shapes=[pltpu.SemaphoreType.DMA((9,))],
        name="finish",
    )(*(pltpu.with_memory_space_constraint(h, vmem) for h in held))
    return (
        mixed, root.reshape(base_state.shape), nv.transpose(1, 0, 2), nb.transpose(1, 0, 2),
        nc.transpose(1, 0, 2), ns,
    )


def solution(mesh):
    return jax.shard_map(
        on_device,
        mesh=mesh,
        in_specs=(
            P("kv", None, "tp"), P(), P("kv", "tp"), P("kv", "tp"), P("kv", "tp"), P("kv", "tp"),
            P(), P(None, "tp"), P(None, "tp"), P(None, "tp"), P("tp"), P("tp"), P("tp"), P("tp"),
            P("tp", "kv"), P("kv", "tp", None, None), P("kv", None, "tp"), P("kv", None, "tp"),
            P("kv", None, "tp"), P("kv", None, "tp"), P("kv"),
        ),
        out_specs=(
            P("kv", None, "tp"), P("kv", "tp", None, None), P("kv", None, "tp"),
            P("kv", None, "tp"), P("kv", None, "tp"), P("kv", None, "tp"),
        ),
        check_vma=False,
    )
```

```python
import jax
import jax.numpy as jnp
from jax import lax
from jax.experimental import pallas as pl
from jax.experimental.pallas import tpu as pltpu
from jax.sharding import PartitionSpec as P

F32 = jnp.float32
BF16 = jnp.bfloat16
MESH = pl.DeviceIdType.MESH
EPSILON = 1e-06
HIGHEST = lax.Precision.HIGHEST

N = 8
SEQ = 4
PROP = 4
ROWS = SEQ * PROP
CONV = 4
PAST = 7
NT = (((1,), (1,)), ((), ()))
TN = (((0,), (0,)), ((), ()))
ORDER = (4, 3, 5, 2, 6, 1, 7)

T1, T2Y, T2Z, WY, WZ, RSY, RSZ, OW, O1, O2 = range(10)
LATE = 22


def silu(v):
    return v / (1.0 + jnp.exp(-v))


def softplus(v):
    return jnp.maximum(v, 0.0) + jnp.log1p(jnp.exp(-jnp.abs(v)))


def conv(buf, taps, at=0):
    total = taps[0:1, :] * buf[at : at + ROWS, :]
    for k in range(1, CONV):
        total = total + taps[k : k + 1, :] * buf[at + SEQ * k : at + SEQ * k + ROWS, :]
    return total


def body(
    tokens, input_gain, gate_w, value_w, write_w, read_w, step_w,
    conv_v, conv_b, conv_c, step_bias, decay_log, skip_gain, output_gain,
    out_w, base, past_v, past_b, past_c, past_s, accepted,
    mixed_m, root_m, nv_m, nb_m, nc_m, ns_m,
    gain_m, stepw_m, cv_m, cb_m, cc_m, bias_m, decay_m, skip_m, og_m,
    base_m, pv_m, pb_m, pc_m, ps_m, tok_m,
    xall, nrm, npk, ay, az, wy, wz, py, pz, rsy, rsz, owg, nrg, po, osum,
    xf, ppv, ppb, ppc, rrv, rrb, rrc, stp, sbuf, ubuf, bbuf, xb, bb, lb, dtb, dj, rootb, mf, nsf,
    taken_m,
    in_sem, send_sem, recv_sem, hello,
):
    kv = lax.axis_index("kv")
    tp = lax.axis_index("tp")
    z = lax.div(kv, N)
    y = lax.rem(kv, N)

    def at(rows, count):
        return pl.ds(pl.multiple_of(rows * count, count), count)

    def up(d):
        return z * N + lax.rem(y + d, N)

    def over(d):
        return (lax.rem(z + d, N)) * N + y

    groups = (
        (
            (value_w, wy.at[at(y, 32), pl.ds(0, 512)]),
            (write_w, wy.at[at(y, 32), pl.ds(512, 128)]),
            (gate_w, wz.at[at(z, 32), pl.ds(0, 512)]),
            (read_w, wz.at[at(z, 32), pl.ds(512, 128)]),
            (out_w, owg.at[at(y, 32), :]),
            (tokens, tok_m),
        ),
        (
            (input_gain, gain_m),
            (past_v, pv_m),
            (past_b, pb_m),
            (past_c, pc_m),
            (conv_v, cv_m),
            (conv_b, cb_m),
            (conv_c, cc_m),
            (output_gain, og_m),
            (step_w, stepw_m),
        ),
        ((past_s, ps_m),),
        ((step_bias, bias_m),),
        ((decay_log, decay_m),),
        ((skip_gain, skip_m),),
        ((accepted, taken_m),),
        ((base, base_m),),
    )
    for i, group in enumerate(groups):
        for source, target in group:
            pltpu.make_async_copy(source, target, in_sem.at[i]).start()

    def loaded(i, ref=None):
        if ref is None:
            pltpu.make_async_copy(*groups[i][0], in_sem.at[i]).wait()
        else:
            pltpu.make_async_copy(ref, ref, in_sem.at[i]).wait()

    barrier = pltpu.get_barrier_semaphore()

    def tell(k, t):
        pl.semaphore_signal(barrier, inc=1, device_id=(k, t), device_id_type=MESH)

    for d in range(1, N):
        tell(kv, lax.rem(tp + d, N))
    for d in (1, 7, 2, 6):
        tell(up(d), tp)
        tell(over(d), tp)

    loaded(0, wy.at[pl.ds(0, 96), :])
    to = lax.broadcasted_iota(jnp.int32, (ROWS, ROWS), 0)
    by = lax.broadcasted_iota(jnp.int32, (ROWS, ROWS), 1)
    swap = jnp.where((to % SEQ) * PROP + to // SEQ == by, 1.0, 0.0).astype(BF16)
    for q in range(SEQ):
        xf[PROP * q : PROP * q + PROP, :] = tok_m[q].astype(F32)
    xall[tp] = jnp.dot(swap, xf[...].astype(BF16), preferred_element_type=F32).astype(BF16)
    pl.semaphore_wait(barrier, N - 1 + 8)
    for d in (2, 6):
        pl.semaphore_signal(hello, inc=1, device_id=(up(d), tp), device_id_type=MESH)
        pl.semaphore_signal(hello, inc=1, device_id=(over(d), tp), device_id_type=MESH)

    def copy(phase, slot, src, dst, k, t):
        return pltpu.make_async_remote_copy(
            src_ref=src, dst_ref=dst, send_sem=send_sem.at[1 if phase in (OW, O1, O2) else 0],
            recv_sem=recv_sem.at[slot],
            device_id=(k, t), device_id_type=MESH,
        )

    def send(phase, src, dst, k, t):
        copy(phase, phase, src, dst, k, t).start()

    def arrived(phase, ref):
        copy(phase, phase, ref, ref, kv, tp).wait_recv()

    def gone(phase, ref):
        copy(phase, phase, ref, ref, kv, tp).wait_send()

    def slab(ref, owner, h):
        return ref.at[pl.ds(pl.multiple_of(owner * 32 + 16 * h, 16), 16), :]

    def pass_slab(phase, slot, ref, owner, h, k):
        copy(phase, slot, slab(ref, owner, h), slab(ref, owner, h), k, tp).start()

    def early(first, h, side):
        return first + 2 * h + side

    def spread_own(rings, steps=((2, 6), (1, 7))):
        for ds in steps:
            for h in range(2):
                for side, d in enumerate(ds):
                    for phase, first, ref, me, dev in rings:
                        slot = early(first, h, side) if d in (2, 6) else phase
                        pass_slab(phase, slot, ref, me, h, dev(d))

    def spread_far(rings):
        for h in range(2):
            for phase, first, ref, me, dev in rings:
                pass_slab(phase, phase, ref, me, h, dev(4))

    def spread_on(rings):
        for h in range(2):
            for side, (back_two, one) in enumerate(((6, 1), (2, 7))):
                for phase, first, ref, me, dev in rings:
                    owner = lax.rem(me + back_two, N)
                    part = slab(ref, owner, h)
                    copy(phase, early(first, h, side), part, part, kv, tp).wait_recv()
                    pass_slab(phase, phase, ref, owner, h, dev(one))

    def spread_end(ring):
        arrived(ring[0], ring[2].at[pl.ds(0, 160), :])

    ring_y = (WY, 10, wy, y, up)
    ring_z = (WZ, 14, wz, z, over)
    ring_o = (OW, 18, owg, y, up)

    for d in range(1, N):
        send(T1, xall.at[tp], xall.at[tp], kv, lax.rem(tp + d, N))
    spread_own((ring_y, ring_z))

    loaded(1, root_m.at[pl.ds(0, 640), :])
    for i in range(2, 8):
        loaded(i)
    for r in range(PAST):
        ppv[SEQ * r : SEQ * r + SEQ, :] = pv_m[r].astype(F32)
        ppb[SEQ * r : SEQ * r + SEQ, :] = pb_m[r].astype(F32)
        ppc[SEQ * r : SEQ * r + SEQ, :] = pc_m[r].astype(F32)

    pl.semaphore_wait(hello, 4)
    spread_far((ring_y, ring_z))

    arrived(T1, xall.at[pl.ds(0, N - 1)])
    blocks = [xall[t].astype(F32) for t in range(N)]
    square = blocks[0] * blocks[0]
    for t in range(1, N):
        square = square + blocks[t] * blocks[t]
    scale = lax.rsqrt(jnp.sum(square, axis=-1, keepdims=True) * (1.0 / 2048) + EPSILON)
    normed = []
    for t in range(N):
        block = (blocks[t] * scale * gain_m[:, 256 * t : 256 * t + 256]).astype(BF16)
        nrm[t] = block
        normed.append(block.astype(F32))
    ay[at(z, ROWS), :] = nrm[z]
    for d in ORDER:
        zz = lax.rem(z + d, N)
        send(T2Y, nrm.at[zz], ay.at[at(z, ROWS), :], over(d), tp)
    lane = lax.broadcasted_iota(jnp.int32, (ROWS, 128), 1) // 32
    for yy in range(N):
        for half in range(2):
            tile = None
            for i in range(4):
                shift = (32 * i - 32 * (yy % 4)) % 128
                start = 128 * (yy // 4)
                piece = normed[4 * half + i][:, start : start + 128]
                if shift:
                    piece = pltpu.roll(piece, shift, 1)
                tile = piece if tile is None else jnp.where(lane == i, piece, tile)
            npk[yy, :, 128 * half : 128 * half + 128] = tile.astype(BF16)
    az[at(y, ROWS), :] = npk[y]
    for d in ORDER:
        yy = lax.rem(y + d, N)
        send(T2Z, npk.at[yy], az.at[at(y, ROWS), :], up(d), tp)
    spread_on((ring_y, ring_z))
    spread_own((ring_o,), ((2, 6),))

    head = lax.broadcasted_iota(jnp.int32, (1, 512), 1) // 64

    def spread(ref):
        row = jnp.zeros((1, 512), F32)
        for h in range(8):
            row = jnp.where(head == h, ref[0:1, h : h + 1], row)
        return row

    bias = spread(bias_m)
    rate = jnp.exp(spread(decay_m))
    skip = spread(skip_m)
    step = jnp.zeros((ROWS, 64), F32)
    for t in range(N):
        weight = stepw_m[:, 256 * t : 256 * t + 256]
        step = step + lax.dot_general(nrm[t], weight, NT, preferred_element_type=F32)
    step16 = step.astype(BF16)
    row64 = lax.broadcasted_iota(jnp.int32, (64, 512), 0)
    own64 = (row64 - 8 * tp == lax.broadcasted_iota(jnp.int32, (64, 512), 1) // 64)
    wide = jnp.dot(step16, jnp.where(own64, 1.0, 0.0).astype(BF16), preferred_element_type=F32)
    row64 = lax.broadcasted_iota(jnp.int32, (64, 128), 0)
    pick = (row64 - 8 * tp == lax.broadcasted_iota(jnp.int32, (64, 128), 1))
    nsf[...] = jnp.dot(step16, jnp.where(pick, 1.0, 0.0).astype(BF16), preferred_element_type=F32)
    for q in range(SEQ):
        ns_m[q] = nsf[pl.ds(q, PROP, stride=SEQ), :][:, 0:8].astype(BF16)

    dt = softplus(wide + bias)
    sbuf[...] = -rate * dt
    run = jnp.zeros((SEQ, 512), F32)
    lb[0:12, :] = jnp.zeros((12, 512), F32)
    dtb[0:12, :] = jnp.zeros((12, 512), F32)
    xb[0:12, :] = jnp.zeros((12, 512), F32)
    bb[0:12, :] = jnp.zeros((12, 128), F32)
    for t in range(PROP):
        run = run + sbuf[SEQ * t : SEQ * t + SEQ, :]
        lb[12 + SEQ * t : 16 + SEQ * t, :] = run
    dtb[12:28, :] = dt
    logs = lb[12:28, :]
    for j in range(PROP):
        lo = 12 - SEQ * j
        dj[j] = jnp.exp(logs - lb[lo : lo + ROWS, :]) * dtb[lo : lo + ROWS, :]

    eight = (
        lax.broadcasted_iota(jnp.int32, (8, 512), 0)
        == lax.broadcasted_iota(jnp.int32, (8, 512), 1) // 64
    )
    eight = jnp.where(eight, 1.0, 0.0).astype(BF16)
    for q in range(SEQ):
        stp[PROP * q : PROP * q + PROP, :] = jnp.dot(
            ps_m[q], eight, preferred_element_type=F32
        )
    steps = jnp.dot(swap, stp[...].astype(BF16), preferred_element_type=F32)
    pd = softplus(steps + bias)

    def taken(shape):
        seq = lax.broadcasted_iota(jnp.int32, shape, 0) % SEQ
        count = jnp.full(shape, taken_m[0], jnp.int32)
        for q in range(1, SEQ):
            count = jnp.where(seq == q, taken_m[q], count)
        return count

    live = lax.broadcasted_iota(jnp.int32, (ROWS, 512), 0) // SEQ < taken((ROWS, 512))
    sbuf[...] = jnp.where(live, -rate * pd, 0.0)
    pls = [sbuf[SEQ * s : SEQ * s + SEQ, :] for s in range(PROP)]
    tails = [None] * PROP
    run = jnp.zeros((SEQ, 512), F32)
    for s in reversed(range(PROP)):
        tails[s] = run
        run = run + pls[s]
    kept = jnp.exp(run)
    for s in range(PROP):
        stp[SEQ * s : SEQ * s + SEQ, :] = jnp.exp(tails[s])
    ubuf[...] = jnp.where(live, stp[...] * pd, 0.0) * silu(conv(ppv, cv_m))
    bbuf[...] = silu(conv(ppb, cb_m))

    def window(pp, rr, width):
        count = taken((12, width))
        first = pp[SEQ : SEQ + 12, :]
        for a in range(2, PROP + 1):
            first = jnp.where(count == a, pp[SEQ * a : SEQ * a + 12, :], first)
        rr[0:12, :] = first

    window(ppv, rrv, 512)
    window(ppb, rrb, 128)
    window(ppc, rrc, 128)

    rest = pl.ds(0, ROWS * (N - 1))

    def others(me):
        return [i + jnp.where(me <= i, 1, 0).astype(jnp.int32) for i in range(N - 1)]

    def sums_y():
        arrived(T2Z, az.at[rest, :])
        spread_end(ring_z)
        pz[...] = jnp.dot(az[...], wz[...], preferred_element_type=F32).astype(BF16)
        for yy in others(y):
            copy(RSZ, RSY, pz.at[at(yy, ROWS), :], rsz.at[y], z * N + yy, tp).start()

    def sums_z():
        arrived(T2Y, ay.at[rest, :])
        spread_end(ring_y)
        py[...] = jnp.dot(ay[...], wy[...], preferred_element_type=F32).astype(BF16)
        for zz in others(z):
            send(RSY, py.at[at(zz, ROWS), :], rsy.at[z], zz * N + y, tp)

    @pl.when(z < 4)
    def _():
        sums_y()
        spread_own((ring_o,), ((1, 7),))
        spread_far((ring_o,))
        sums_z()

    @pl.when(z >= 4)
    def _():
        sums_z()
        sums_y()
        spread_own((ring_o,), ((1, 7),))
        spread_far((ring_o,))

    rsy[z] = py[at(z, ROWS), :]
    rsz[y] = pz[at(y, ROWS), :]

    seq = lax.broadcasted_iota(jnp.int32, (ROWS, 512), 0) % SEQ
    for q in range(SEQ):
        u = jnp.where(seq == q, ubuf[...], 0.0)
        grown = lax.dot_general(u, bbuf[...], TN, precision=HIGHEST, preferred_element_type=F32)
        for h in range(8):
            lo = 512 * q + 64 * h
            old = jnp.broadcast_to(kept[q : q + 1, 64 * h : 64 * h + 1], (64, 128))
            new = old * base_m[lo : lo + 64, :] + grown[64 * h : 64 * h + 64, :]
            root_m[lo : lo + 64, :] = new
            rootb[lo : lo + 64, :] = new.astype(BF16)

    spread_on((ring_o,))

    arrived(RSY, wy.at[pl.ds(0, 224), :])

    def summed(ref, lo, hi):
        total = ref[0, :, lo:hi].astype(F32)
        for s in range(1, N):
            total = total + ref[s, :, lo:hi].astype(F32)
        return total.astype(BF16).astype(F32)

    rrv[12:28, :] = summed(rsy, 0, 512)
    rrb[12:28, :] = summed(rsy, 512, 640)
    rrc[12:28, :] = summed(rsz, 512, 640)
    gate = summed(rsz, 0, 512)
    x = silu(conv(rrv, cv_m))
    b = silu(conv(rrb, cb_m))
    c = silu(conv(rrc, cc_m))
    xb[12:28, :] = x
    bb[12:28, :] = b
    c16 = c.astype(BF16)
    carried = jnp.zeros((ROWS, 512), F32)
    for q in range(SEQ):
        one = lax.dot_general(
            c16, rootb[512 * q : 512 * q + 512, :], NT, preferred_element_type=F32
        )
        carried = jnp.where(seq == q, one, carried)
    out = jnp.exp(logs) * carried + skip * x
    for j in range(PROP):
        lo = 12 - SEQ * j
        score = jnp.sum(c * bb[lo : lo + ROWS, :], axis=-1, keepdims=True)
        out = out + score * dj[j] * xb[lo : lo + ROWS, :]
    g = out * silu(gate)
    g = g * lax.rsqrt(jnp.mean(g * g, axis=-1, keepdims=True) + EPSILON)
    nrg[at(z, ROWS), :] = (g * og_m[...]).astype(BF16)
    slot = LATE + jnp.where(z < 2, z, lax.div(z, 2) + 1).astype(jnp.int32)
    for d in ORDER:
        copy(O1, slot, nrg.at[at(z, ROWS), :], nrg.at[at(z, ROWS), :], over(d), tp).start()
    for r in range(PAST):
        nv_m[r] = rrv[SEQ * r : SEQ * r + SEQ, :].astype(BF16)
        nb_m[r] = rrb[SEQ * r : SEQ * r + SEQ, :].astype(BF16)
        nc_m[r] = rrc[SEQ * r : SEQ * r + SEQ, :].astype(BF16)

    spread_end(ring_o)
    for i, (low, high) in enumerate(((0, 1), (1, 2), (2, 4), (4, 6), (6, 8))):
        mine = jnp.logical_and(z >= low, z < high)
        sem = LATE + i

        def landed(count):
            if count:
                some = nrg.at[pl.ds(0, count * ROWS), :]
                copy(O1, sem, some, some, kv, tp).wait_recv()

        if high - low > 1:

            @pl.when(mine)
            def _():
                landed(high - low - 1)

        @pl.when(jnp.logical_not(mine))
        def _():
            landed(high - low)

        part = pl.ds(ROWS * low, ROWS * (high - low))
        po[part, :] = lax.dot_general(
            nrg[part, :], owg[...], NT, preferred_element_type=F32
        ).astype(BF16)
        for zz in range(low, high):
            local = jnp.logical_and(z == zz, tp == zz)

            @pl.when(jnp.logical_not(local))
            def _():
                send(O2, po.at[pl.ds(ROWS * zz, ROWS), :], osum.at[tp], zz * N + y, z)

            @pl.when(local)
            def _():
                osum[tp] = po[ROWS * zz : ROWS * zz + ROWS, :]

    @pl.when(z != tp)
    def _():
        arrived(O2, osum)

    @pl.when(z == tp)
    def _():
        arrived(O2, osum.at[pl.ds(0, N - 1)])

    total = osum[0].astype(F32)
    for t in range(1, N):
        total = total + osum[t].astype(F32)
    for i in range(2):
        mf[i] = total[:, 128 * i : 128 * i + 128]
        for q in range(SEQ):
            mixed_m[q, :, 128 * i : 128 * i + 128] = mf.at[i][
                pl.ds(q, PROP, stride=SEQ), :
            ].astype(BF16)

    gone(T1, base_m.at[pl.ds(0, 2016), :])

    @pl.when(z != tp)
    def _():
        gone(O2, base_m.at[pl.ds(0, 800), :])

    @pl.when(z == tp)
    def _():
        gone(O2, base_m.at[pl.ds(0, 784), :])


def finish(*refs):
    ins, outs, sem = refs[:6], refs[6:12], refs[12]
    parts = [pl.ds(256 * i, 256) for i in range(8)]
    pairs = [(ins[1].at[part], outs[1].at[part]) for part in parts]
    pairs += [(s, d) for i, (s, d) in enumerate(zip(ins, outs)) if i != 1]
    copies = [pltpu.make_async_copy(s, d, sem.at[i]) for i, (s, d) in enumerate(pairs)]
    for c in copies:
        c.start()
    for c in copies:
        c.wait()


def on_device(
    tokens, input_gain, gate_weight, value_weight, write_weight, read_weight, step_weight,
    conv_value, conv_write, conv_read, step_bias, decay_log, skip_gain, output_gain,
    out_weight, base_state, past_value, past_write, past_read, past_step, accepted,
):
    vmem = pltpu.VMEM
    ops = (
        tokens, input_gain[None, :], gate_weight, value_weight, write_weight, read_weight,
        step_weight.T, conv_value, conv_write, conv_read, step_bias[None, :],
        decay_log[None, :], skip_gain[None, :], output_gain[None, :], out_weight.T,
        base_state.reshape(2048, 128), past_value.transpose(1, 0, 2),
        past_write.transpose(1, 0, 2), past_read.transpose(1, 0, 2), past_step, accepted,
    )
    out_shapes = [
        ((SEQ, PROP, 256), BF16), ((2048, 128), F32), ((PAST, SEQ, 512), BF16),
        ((PAST, SEQ, 128), BF16), ((PAST, SEQ, 128), BF16), ((SEQ, PROP, 8), BF16),
    ]
    scratch = [
        vmem((1, 2048), F32), vmem((64, 2048), BF16), vmem((4, 512), F32), vmem((4, 128), F32),
        vmem((4, 128), F32), vmem((1, 8), F32), vmem((1, 8), F32), vmem((1, 8), F32),
        vmem((1, 512), F32), vmem((2048, 128), F32), vmem((PAST, SEQ, 512), BF16),
        vmem((PAST, SEQ, 128), BF16), vmem((PAST, SEQ, 128), BF16), vmem((SEQ, PROP, 8), BF16),
        vmem((SEQ, PROP, 256), BF16),
        vmem((N, ROWS, 256), BF16), vmem((N, ROWS, 256), BF16), vmem((N, ROWS, 256), BF16),
        vmem((128, 256), BF16), vmem((128, 256), BF16), vmem((256, 640), BF16),
        vmem((256, 640), BF16), vmem((128, 640), BF16), vmem((128, 640), BF16),
        vmem((N, ROWS, 640), BF16), vmem((N, ROWS, 640), BF16), vmem((256, 512), BF16),
        vmem((128, 512), BF16), vmem((128, 256), BF16), vmem((N, ROWS, 256), BF16),
        vmem((ROWS, 256), F32), vmem((28, 512), F32), vmem((28, 128), F32), vmem((28, 128), F32),
        vmem((28, 512), F32), vmem((28, 128), F32), vmem((28, 128), F32), vmem((ROWS, 512), F32),
        vmem((ROWS, 512), F32), vmem((ROWS, 512), F32), vmem((ROWS, 128), F32),
        vmem((28, 512), F32), vmem((28, 128), F32), vmem((28, 512), F32), vmem((28, 512), F32),
        vmem((PROP, ROWS, 512), F32), vmem((2048, 128), BF16), vmem((2, ROWS, 128), F32),
        vmem((ROWS, 128), F32),
        pltpu.SMEM((SEQ,), jnp.int32),
        pltpu.SemaphoreType.DMA((8,)),
        pltpu.SemaphoreType.DMA((2,)),
        pltpu.SemaphoreType.DMA((27,)),
        pltpu.SemaphoreType.REGULAR,
    ]
    held = pl.pallas_call(
        body,
        out_shape=[vmem(shape, dtype) for shape, dtype in out_shapes],
        in_specs=[pl.BlockSpec(memory_space=pl.ANY)] * 21,
        out_specs=[pl.BlockSpec(memory_space=vmem)] * 6,
        scratch_shapes=scratch,
        compiler_params=pltpu.CompilerParams(collective_id=0, has_side_effects=True),
        name="mixer",
    )(*ops)
    mixed, root, nv, nb, nc, ns = pl.pallas_call(
        finish,
        out_shape=[jax.ShapeDtypeStruct(shape, dtype) for shape, dtype in out_shapes],
        in_specs=[pl.BlockSpec(memory_space=vmem)] * 6,
        out_specs=[pl.BlockSpec(memory_space=pl.ANY)] * 6,
        scratch_shapes=[pltpu.SemaphoreType.DMA((13,))],
        name="finish",
    )(*(pltpu.with_memory_space_constraint(h, vmem) for h in held))
    return (
        mixed, root.reshape(base_state.shape), nv.transpose(1, 0, 2), nb.transpose(1, 0, 2),
        nc.transpose(1, 0, 2), ns,
    )


def solution(mesh):
    return jax.shard_map(
        on_device,
        mesh=mesh,
        in_specs=(
            P("kv", None, "tp"), P(), P("kv", "tp"), P("kv", "tp"), P("kv", "tp"), P("kv", "tp"),
            P(), P(None, "tp"), P(None, "tp"), P(None, "tp"), P("tp"), P("tp"), P("tp"), P("tp"),
            P("tp", "kv"), P("kv", "tp", None, None), P("kv", None, "tp"), P("kv", None, "tp"),
            P("kv", None, "tp"), P("kv", None, "tp"), P("kv"),
        ),
        out_specs=(
            P("kv", None, "tp"), P("kv", "tp", None, None), P("kv", None, "tp"),
            P("kv", None, "tp"), P("kv", None, "tp"), P("kv", None, "tp"),
        ),
        check_vma=False,
    )
```
